128 devices in a mesh: sp: 16 (over z, y), dp: 8 (over x, core).
Axes of the slice: x: 4, y: 4, z: 4, core: 2. Of those that a mesh axis runs over, the one named last changes fastest.
Arguments:
- queries: bfloat16 [8, 2048, 2048], P('dp', 'sp'), may hold values from -40 to 40
- keys: bfloat16 [8, 2048, 512], P('dp', 'sp'), may hold values from -8 to 8
- values: bfloat16 [8, 2048, 512], P('dp', 'sp'), may hold values from -6 to 6
- lambdas: float32 [16], replicated, may hold values from 0.3 to 0.8
- value_gain: float32 [128], replicated, may hold values from 0.1 to 1.9
- out_weight: bfloat16 [2048, 4096], P(None, ('sp', 'dp')), may hold values from -0.125 to 0.125
Outputs:
- mixed: bfloat16 [8, 2048, 4096], P('dp', 'sp')
The draws below stay inside these ranges and needn't reach their ends.
All inputs are finite; a program needn't handle non-finite values.
Results may differ from the reference program's by a relative error of at most 0.0087.
Values may be sent and summed in bfloat16 or wider, within the bound.
A program may use at most 128 MiB of HBM per device.

```python
import jax
import jax.numpy as jnp
from jax import lax

D = 4096
HEADS = 16
KV_HEADS = 4
HEAD_DIM = 64
VALUE_DIM = 128
SEQLEN = 2048
SEQS = 8


def base_keys(key):
    draw_key = jax.random.fold_in(key, 3)
    shape = (SEQS, SEQLEN, KV_HEADS, 2, HEAD_DIM)
    keys_float = jnp.clip(1.3 * jax.random.normal(draw_key, shape, jnp.float32), -8.0, 8.0)
    return keys_float


def draw_keys(key, part):
    return base_keys(key).reshape(SEQS, SEQLEN, KV_HEADS * 2 * HEAD_DIM).astype(jnp.bfloat16)


def draw_queries(key, part):
    draw_key = jax.random.fold_in(key, 4)
    shape = (SEQS, SEQLEN, HEADS, 2, HEAD_DIM)
    queries_float = jnp.clip(1.3 * jax.random.normal(draw_key, shape, jnp.float32), -8.0, 8.0)
    return queries_float.reshape(SEQS, SEQLEN, HEADS * 2 * HEAD_DIM).astype(jnp.bfloat16)


def block_levels(own_key, shape, pieces, low, high):
    loudness = 1.0
    for position, blocks in pieces:
        steps = jax.random.uniform(jax.random.fold_in(jax.random.fold_in(own_key, 6), position), (blocks,), jnp.float32, low / len(pieces), high / len(pieces))
        loudness = loudness * jnp.repeat(jnp.exp(steps), shape[position] // blocks).reshape((-1,) + (1,) * (len(shape) - 1 - position))
    return loudness


def scatter_about(own_key, extent, deviation, most, split=(), kind=jnp.bfloat16):
    result = deviation * jax.random.normal(own_key, extent, jnp.float32)
    if split:
        result = result * block_levels(own_key, extent, split, -0.22, 0.18)
    return jnp.clip(result, -most, most).astype(kind)


def setup_inputs(seed: int = 0) -> dict:
    key_of = jax.random.split(jax.random.key(seed), 7)
    queries = draw_queries(jax.random.fold_in(key_of[6], 71), 0)
    keys = draw_keys(jax.random.fold_in(key_of[6], 71), 0)
    values = scatter_about(key_of[2], (SEQS, SEQLEN, KV_HEADS * VALUE_DIM), 1.0, 6.0, ((0, 8), (1, 16)))
    lambdas = jnp.clip(jax.random.uniform(key_of[3], (HEADS,), jnp.float32, 0.3, 0.8), 0.3, 0.8)
    value_gain = jnp.clip(1.0 + 0.18 * jax.random.normal(key_of[4], (VALUE_DIM,), jnp.float32), 0.1, 1.9)
    out_weight = scatter_about(key_of[5], (HEADS * VALUE_DIM, D), (HEADS * VALUE_DIM) ** -0.5, 0.125, ((1, 128),))
    return {"queries": queries, "keys": keys, "values": values, "lambdas": lambdas, "value_gain": value_gain, "out_weight": out_weight}


rope_base = 500000.0
output_scale = 0.8
norm_eps = 1e-05

def rotate_all(parts, positions):
    width = parts.shape[-1]
    half = width // 2
    freqs = rope_base ** (-jnp.arange(0, width, 2, dtype=jnp.float32) / width)
    angles = positions[:, None] * freqs[None, :]
    shape = (1, angles.shape[0], 1, 1, half)
    cosine = jnp.cos(angles).reshape(shape)
    sine = jnp.sin(angles).reshape(shape)
    first = parts[..., :half]
    second = parts[..., half:]
    return jnp.concatenate([first * cosine - second * sine, second * cosine + first * sine], -1)

def reference(queries, keys, values, lambdas, value_gain, out_weight):
    positions = jnp.arange(SEQLEN, dtype=jnp.float32)
    query_rot = rotate_all(queries.astype(jnp.float32).reshape(SEQS, SEQLEN, HEADS, 2, HEAD_DIM), positions).astype(jnp.bfloat16)
    key_rot = rotate_all(keys.astype(jnp.float32).reshape(SEQS, SEQLEN, KV_HEADS, 2, HEAD_DIM), positions).astype(jnp.bfloat16)
    value_parts = values.reshape(SEQS, SEQLEN, KV_HEADS, VALUE_DIM)
    group_size = HEADS // KV_HEADS
    key_heads = jnp.repeat(key_rot, group_size, axis=2)
    value_heads = jnp.repeat(value_parts, group_size, axis=2)
    query_flat = jnp.transpose(query_rot, (0, 2, 1, 3, 4)).reshape(SEQS * HEADS, SEQLEN, 2, HEAD_DIM)
    key_flat = jnp.transpose(key_heads, (0, 2, 1, 3, 4)).reshape(SEQS * HEADS, SEQLEN, 2, HEAD_DIM)
    value_flat = jnp.transpose(value_heads, (0, 2, 1, 3)).reshape(SEQS * HEADS, SEQLEN, VALUE_DIM)
    lambda_flat = jnp.tile(lambdas, SEQS)
    block_rows = min(512, SEQLEN)
    count = SEQLEN // block_rows
    score_scale = HEAD_DIM ** (-0.5)
    key_places = jnp.arange(SEQLEN)

    def one_head(inputs):
        query_one, key_one, value_one, lambda_one = inputs

        def one_block(block_index):
            start = block_index * block_rows
            query_block = lax.dynamic_slice_in_dim(query_one, start, block_rows, 0)
            scores = jnp.einsum('qmd,kmd->mqk', query_block.astype(jnp.float32), key_one.astype(jnp.float32)) * score_scale
            allowed = key_places[None, :] <= (start + jnp.arange(block_rows))[:, None]
            scores = jnp.where(allowed[None], scores, -jnp.inf)
            row_top = lax.optimization_barrier(jnp.max(scores, -1, keepdims=True))
            raised = jnp.exp(scores - row_top)
            maps = raised / lax.optimization_barrier(jnp.sum(raised, -1, keepdims=True))
            weights = (maps[0] - lambda_one * maps[1]).astype(jnp.bfloat16)
            return jnp.dot(weights, value_one, preferred_element_type=jnp.float32)
        blocks = lax.map(one_block, jnp.arange(count))
        head_values = blocks.reshape(SEQLEN, VALUE_DIM)
        squares = lax.optimization_barrier(jnp.mean(head_values * head_values, -1, keepdims=True))
        return (head_values * lax.rsqrt(squares + norm_eps) * value_gain * output_scale).astype(jnp.bfloat16)
    head_out = lax.map(one_head, (query_flat, key_flat, value_flat, lambda_flat))
    heads_out = jnp.transpose(head_out.reshape(SEQS, HEADS, SEQLEN, VALUE_DIM), (0, 2, 1, 3)).reshape(SEQS * SEQLEN, HEADS * VALUE_DIM)
    mixed = jnp.dot(heads_out, out_weight, preferred_element_type=jnp.float32).astype(jnp.bfloat16)
    return mixed.reshape(SEQS, SEQLEN, D)
```

```python
import functools

import jax
import jax.numpy as jnp
import numpy as np
from jax import lax
from jax.experimental import pallas as pl
from jax.experimental.pallas import tpu as pltpu
from jax.sharding import PartitionSpec as P

HEADS = 16
KV_HEADS = 4
HEAD_DIM = 64
VALUE_DIM = 128
D = 4096
SEQLEN = 2048
ROWS = 128
GROUP = HEADS // KV_HEADS
KT = 256
ROPE_BASE = 500000.0
OUTPUT_SCALE = 0.8
NORM_EPS = 1e-05
MESH = pl.DeviceIdType.MESH

COLOURS = (
    (("y", "z", "x"), 0, 1024),
    (("x", "z", "y"), 1024, 768),
    (("x", "y", "z"), 1792, 256),
)


def rotation_tables():
    f32 = np.float32
    freqs = (f32(ROPE_BASE) ** (-np.arange(0, HEAD_DIM, 2, dtype=f32) / f32(HEAD_DIM))).astype(f32)
    lanes = np.tile(freqs.astype(np.float64), 4)
    inner = np.arange(ROWS)[:, None] * lanes[None]
    outer = (np.arange(SEQLEN // ROWS) * ROWS)[:, None] * lanes[None]
    inner = np.stack([np.cos(inner), np.sin(inner)]).astype(f32)
    outer = np.stack([np.cos(outer), np.sin(outer)], 1).astype(f32)
    return inner, outer


def kernel(
    lam_ref, q_hbm, k_hbm, v_hbm, gain_ref, inner_ref, outer_ref, w_hbm,
    out_ref,
    q_in, k_in, v_in, kvst, kv, qst, qin, q2, sbuf, acc, wbuf, hst, acts, oown, opart, oin,
    in_sem, kvz_s, kvz_r, kvy_s, kvy_r, qz_s, qz_r, w_s, w_r, oz_s, oz_r, af_s, af_r, oo_s, oo_r,
):
    f32, bf16 = jnp.float32, jnp.bfloat16
    sp, dp = lax.axis_index("sp"), lax.axis_index("dp")
    me = {"z": sp // 4, "y": lax.rem(sp, 4), "x": dp // 2}
    core = lax.rem(dp, 2)

    def at(pos):
        return (pos["z"] * 4 + pos["y"], pos["x"] * 2 + core)

    def shift(dim, off):
        return {**me, dim: lax.rem(me[dim] + off + 4, 4)}

    partner = (sp, me["x"] * 2 + 1 - core)
    pending = []

    def send(src, dst, s_sem, r_sem, dev):
        copy = pltpu.make_async_remote_copy(
            src_ref=src, dst_ref=dst, send_sem=s_sem, recv_sem=r_sem, device_id=dev, device_id_type=MESH
        )
        copy.start()
        pending.append(copy)

    def arrived(dst, s_sem, r_sem):
        pltpu.make_async_remote_copy(
            src_ref=dst, dst_ref=dst, send_sem=s_sem, recv_sem=r_sem, device_id=partner, device_id_type=MESH
        ).wait_recv()

    c_k = pltpu.make_async_copy(k_hbm, k_in, in_sem.at[0])
    c_v = pltpu.make_async_copy(v_hbm, v_in, in_sem.at[1])
    c_w = pltpu.make_async_copy(w_hbm, wbuf.at[me["z"], me["y"], me["x"]], in_sem.at[2])
    c_q = pltpu.make_async_copy(q_hbm, q_in, in_sem.at[3])
    for c in (c_k, c_v, c_w, c_q):
        c.start()

    barrier = pltpu.get_barrier_semaphore()
    peers = [at(shift("z", o)) for o in (1, 2, 3)] + [at(shift("y", o)) for o in (1, 3)]
    peers += [at(shift("x", o)) for o in (1, 3)] + [partner]
    for dev in peers:
        pl.semaphore_signal(barrier, inc=1, device_id=dev, device_id_type=MESH)

    ci, si = inner_ref[0], inner_ref[1]
    co, so = outer_ref[sp, 0:1, :], outer_ref[sp, 1:2, :]
    cosine = co * ci - so * si
    sine = so * ci + co * si
    row = lax.broadcasted_iota(jnp.int32, (128, 128), 0)
    col = lax.broadcasted_iota(jnp.int32, (128, 128), 1)
    low = lax.rem(col, 64) < 32
    swap = jnp.where(
        low & (row == col + 32), -1.0, jnp.where(jnp.logical_not(low) & (row == col - 32), 1.0, 0.0)
    ).astype(bf16)

    def rotate(part):
        turned = jnp.dot(part, swap, preferred_element_type=f32)
        return (part.astype(f32) * cosine + turned * sine).astype(bf16)

    c_k.wait()
    c_v.wait()
    for g in range(KV_HEADS):
        cols = slice(g * 128, (g + 1) * 128)
        kvst[g, 0] = rotate(k_in[:, cols])
        kvst[g, 1] = v_in[:, cols].astype(f32).T.astype(bf16)
    kv[sp, 0] = kvst[me["z"], 0]
    kv[sp, 1] = kvst[me["z"], 1]
    pl.semaphore_wait(barrier, len(peers))

    for o in (1, 3, 2):
        pos = shift("z", o)
        send(kvst.at[pos["z"]], kv.at[sp], kvz_s.at[o - 1], kvz_r.at[o - 1], at(pos))

    def kv_block(rel, off):
        return lax.rem(me["z"] + rel, 4) * 4 + lax.rem(me["y"] + off + 4, 4)

    def kvy_start(rel):
        view = kvst.at[me["z"]] if rel == 0 else kv.at[kv_block(rel, 0)]
        dst = kv.at[kv_block(rel, 0)]
        for slot, off in ((0, 1), (1, -1)):
            send(view, dst, kvy_s.at[rel * 4 + slot], kvy_r.at[rel * 4 + slot], at(shift("y", off)))

    def kvy_forward(rel):
        for slot, off in ((0, -1), (1, 1)):
            view = kv.at[kv_block(rel, off)]
            arrived(view, kvy_s.at[rel * 4 + slot], kvy_r.at[rel * 4 + slot])
            half = kv.at[kv_block(rel, off), slot]
            n = rel * 4 + slot + 2
            send(half, half, kvy_s.at[n], kvy_r.at[n], at(shift("y", -off)))

    def kvy_finish(rel):
        for slot in (0, 1):
            n = rel * 4 + slot + 2
            arrived(kv.at[kv_block(rel, 2), slot], kvy_s.at[n], kvy_r.at[n])

    def kvz_wait(rel):
        o = 4 - rel
        arrived(kv.at[kv_block(rel, 0)], kvz_s.at[o - 1], kvz_r.at[o - 1])

    kvy_start(0)

    def wview(ci_, phase, b1=None, b2=None, b3=None, half=None):
        order, k0, kn = COLOURS[ci_]
        sel = dict(me)
        rows = slice(None)
        if phase == 1:
            sel[order[0]] = b1
            if half is not None:
                rows = pl.ds(16 * half, 16)
        else:
            sel[order[0]] = slice(None) if half is None else pl.ds(2 * half, 2)
            sel[order[1]] = b2
            if phase == 3:
                sel[order[2]] = b3
        return wbuf.at[sel["z"], sel["y"], sel["x"], rows, pl.ds(k0, kn)]

    class Ring:
        def __init__(self, ci_, phase, rel=0):
            self.ci, self.phase, self.rel = ci_, phase, rel
            self.dim = COLOURS[ci_][0][phase - 1]
            self.base = ci_ * 24 + (phase - 1 + rel if phase == 3 else phase - 1) * 4

        def view(self, off, half=None):
            spot = lax.rem(me[self.dim] + off + 4, 4)
            if self.phase == 1:
                return wview(self.ci, 1, b1=spot, half=half)
            if self.phase == 2:
                return wview(self.ci, 2, b2=spot, half=half)
            other = COLOURS[self.ci][0][1]
            return wview(self.ci, 3, b2=lax.rem(me[other] + self.rel, 4), b3=spot, half=half)

        def start(self):
            view = self.view(0)
            for slot, off in ((0, 1), (1, -1)):
                n = self.base + slot
                send(view, view, w_s.at[n], w_r.at[n], at(shift(self.dim, off)))

        def forward(self, slot):
            off = (-1, 1)[slot]
            n = self.base + slot
            arrived(self.view(off), w_s.at[n], w_r.at[n])
            half = self.view(off, slot)
            send(half, half, w_s.at[n + 2], w_r.at[n + 2], at(shift(self.dim, -off)))

        def finish(self):
            for slot in (0, 1):
                n = self.base + slot + 2
                arrived(self.view(2, slot), w_s.at[n], w_r.at[n])

    p1 = [Ring(c, 1) for c in range(3)]
    p2 = [Ring(c, 2) for c in range(3)]
    p3 = [[Ring(c, 3, r) for r in range(4)] for c in range(3)]

    c_w.wait()
    for c in range(3):
        p1[c].start()

    c_q.wait()
    for g in range(KV_HEADS):
        for h in range(GROUP):
            a = (g * GROUP + h) * 128
            qst[g, :, h * 128:(h + 1) * 128] = rotate(q_in[:, a:a + 128])
    for o in (1, 3, 2):
        pos = shift("z", o)
        send(qst.at[pos["z"]], qin.at[me["z"]], qz_s.at[o - 1], qz_r.at[o - 1], at(pos))
    qin[me["z"]] = qst[me["z"]]

    kvz_wait(3)
    kvy_start(3)
    kvz_wait(1)
    kvy_start(1)
    kvy_forward(0)
    for c in range(3):
        p1[c].forward(0)
        p1[c].forward(1)
    kvz_wait(2)
    kvy_start(2)
    kvy_forward(3)
    kvy_forward(1)
    for c in range(3):
        p1[c].finish()
        p2[c].start()
        p3[c][0].start()
    kvy_forward(2)
    for rel in (0, 3, 1, 2):
        kvy_finish(rel)

    scale = float(HEAD_DIM ** -0.5 * np.log2(np.e))
    lam = jnp.concatenate(
        [jnp.full((1, 128), lam_ref[me["z"] * GROUP + h], f32) for h in range(GROUP)], 1
    )
    lane = lax.broadcasted_iota(jnp.int32, (128, 128), 1)
    half_rows = GROUP * ROWS

    def attend(i):
        zq = lax.rem(me["z"] + 1 + i, 4)
        if i < 3:
            o = 3 - i
            arrived(qin.at[zq], qz_s.at[o - 1], qz_r.at[o - 1])
        for m in range(2):
            keep = (lane < 64) if m == 0 else (lane >= 64)
            for h in range(GROUP):
                part = qin[zq, :, h * 128:(h + 1) * 128]
                q2[(m * GROUP + h) * 128:(m * GROUP + h + 1) * 128, :] = jnp.where(
                    keep, part, jnp.zeros_like(part)
                )
        block = zq * 4 + me["y"]
        last = block // 2

        def scores(t):
            keys = jnp.concatenate([kv[2 * t, 0], kv[2 * t + 1, 0]], 0)
            return lax.dot_general(keys, q2[...], (((1,), (1,)), ((), ())), preferred_element_type=f32)

        def fold(x, op):
            r = x.reshape(KT // 8, 8, x.shape[1])
            return op(r, 0)

        def pass1(t, top):
            s = scores(t)
            sbuf[t] = s
            return jnp.maximum(top, fold(s, jnp.max))

        top = lax.fori_loop(0, last, pass1, jnp.full((8, 2 * half_rows), -1e30, f32))
        s = scores(last)
        key_at = lax.broadcasted_iota(jnp.int32, (KT, 2 * half_rows), 0) + last * KT
        query_at = lax.rem(lax.broadcasted_iota(jnp.int32, (KT, 2 * half_rows), 1), 128) + block * 128
        s = jnp.where(key_at <= query_at, s, -1e30)
        sbuf[last] = s
        top = jnp.maximum(top, fold(s, jnp.max))
        top = jnp.max(top, 0, keepdims=True)

        def pass2(t, total):
            p = jnp.exp2((sbuf[t] - top) * scale)
            sbuf[t] = p
            return total + fold(p, jnp.sum)

        total = lax.fori_loop(0, last + 1, pass2, jnp.zeros((8, 2 * half_rows), f32))
        total = jnp.sum(total, 0, keepdims=True)
        a0 = 1.0 / total[:, :half_rows]
        a1 = lam / total[:, half_rows:]
        acc[...] = jnp.zeros_like(acc)

        def pass3(t, carry):
            w = (sbuf[t, :, :half_rows] * a0 - sbuf[t, :, half_rows:] * a1).astype(bf16)
            vals = jnp.concatenate([kv[2 * t, 1], kv[2 * t + 1, 1]], 1)
            acc[...] += jnp.dot(vals, w, preferred_element_type=f32)
            return carry

        lax.fori_loop(0, last + 1, pass3, 0)
        hv = acc[...]
        inv = lax.rsqrt(jnp.mean(hv * hv, 0, keepdims=True) + NORM_EPS)
        hv = hv * inv
        for h in range(GROUP):
            piece = hv[:, h * 128:(h + 1) * 128].T
            hst[zq, :, h * 128:(h + 1) * 128] = (piece * gain_ref[...] * OUTPUT_SCALE).astype(bf16)
        return zq

    def ship(i, zq):
        if i < 3:
            o = i + 1
            send(hst.at[zq], acts.at[0, me["z"]], oz_s.at[o - 1], oz_r.at[o - 1], at(shift("z", o)))
        else:
            acts[0, me["z"]] = hst[me["z"]]
            send(hst.at[me["z"]], acts.at[1, me["z"]], af_s.at[3], af_r.at[3], partner)

    zq = attend(0)
    ship(0, zq)
    for c in range(3):
        p2[c].forward(0)
        p3[c][3].start()
    zq = attend(1)
    ship(1, zq)
    for c in range(3):
        p2[c].forward(1)
        p3[c][1].start()
    zq = attend(2)
    ship(2, zq)
    for c in range(3):
        p3[c][0].forward(0)
        p3[c][0].forward(1)
        p2[c].finish()
        p3[c][2].start()
    zq = attend(3)
    ship(3, zq)
    for o in (1, 2, 3):
        g = lax.rem(me["z"] + 4 - o, 4)
        arrived(acts.at[0, g], oz_s.at[o - 1], oz_r.at[o - 1])
        send(acts.at[0, g], acts.at[1, g], af_s.at[o - 1], af_r.at[o - 1], partner)
    for r in (3, 1, 2):
        for c in range(3):
            p3[c][r].forward(0)
            p3[c][r].forward(1)
    for o in (1, 2, 3):
        g = lax.rem(me["z"] + 4 - o, 4)
        arrived(acts.at[1, g], af_s.at[o - 1], af_r.at[o - 1])
    arrived(acts.at[1, me["z"]], af_s.at[3], af_r.at[3])
    for r in (0, 3, 1, 2):
        for c in range(3):
            p3[c][r].finish()

    def project(n):
        total = None
        weights = wbuf[n].reshape(512, 2048)
        for g in range(KV_HEADS):
            left = acts[:, g].reshape(2 * ROWS, 512)
            part = lax.dot_general(
                left, weights[:, g * 512:(g + 1) * 512], (((1,), (1,)), ((), ())), preferred_element_type=f32
            )
            total = part if total is None else total + part
        oown[n] = total[:ROWS].astype(bf16)
        opart[n] = total[ROWS:].astype(bf16)

    for n in range(4):
        project(n)
        send(opart.at[n], oin.at[n], oo_s.at[n], oo_r.at[n], partner)

    erow = lax.broadcasted_iota(jnp.int32, (256, 256), 0)
    ecol = lax.broadcasted_iota(jnp.int32, (256, 256), 1)
    mine = jnp.where(erow < 128, core, 1 - core)
    er = lax.rem(erow, 128)
    spread = jnp.where(ecol == (er // 32) * 64 + mine * 32 + lax.rem(er, 32), 1.0, 0.0).astype(bf16)
    for n in range(4):
        arrived(oin.at[n], oo_s.at[n], oo_r.at[n])
        for b in range(4):
            both = jnp.concatenate([oown[n, :, b * 128:(b + 1) * 128], oin[n, :, b * 128:(b + 1) * 128]], 1)
            a = (n * 4 + b) * 256
            out_ref[:, a:a + 256] = jnp.dot(both, spread, preferred_element_type=f32).astype(bf16)
    for copy in pending:
        copy.wait_send()


def shards(queries, keys, values, lambdas, value_gain, out_weight):
    inner, outer = rotation_tables()
    vmem = pl.BlockSpec(memory_space=pltpu.VMEM)
    smem = pl.BlockSpec(memory_space=pltpu.SMEM)
    hbm = pl.BlockSpec(memory_space=pl.ANY)
    bf16, f32 = jnp.bfloat16, jnp.float32
    dma = lambda n: pltpu.SemaphoreType.DMA((n,))
    out = pl.pallas_call(
        kernel,
        out_shape=jax.ShapeDtypeStruct((ROWS, D), bf16),
        in_specs=[smem, hbm, hbm, hbm, vmem, vmem, vmem, hbm],
        out_specs=vmem,
        scratch_shapes=[
            pltpu.VMEM((ROWS, 2048), bf16),
            pltpu.VMEM((ROWS, 512), bf16),
            pltpu.VMEM((ROWS, 512), bf16),
            pltpu.VMEM((4, 2, 128, 128), bf16),
            pltpu.VMEM((16, 2, 128, 128), bf16),
            pltpu.VMEM((4, 128, 512), bf16),
            pltpu.VMEM((4, 128, 512), bf16),
            pltpu.VMEM((1024, 128), bf16),
            pltpu.VMEM((8, KT, 1024), f32),
            pltpu.VMEM((128, 512), f32),
            pltpu.VMEM((4, 4, 4, 32, 2048), bf16),
            pltpu.VMEM((4, 128, 512), bf16),
            pltpu.VMEM((2, 4, 128, 512), bf16),
            pltpu.VMEM((4, 128, 512), bf16),
            pltpu.VMEM((4, 128, 512), bf16),
            pltpu.VMEM((4, 128, 512), bf16),
            dma(4), dma(3), dma(3), dma(16), dma(16), dma(3), dma(3), dma(72), dma(72),
            dma(3), dma(3), dma(4), dma(4), dma(4), dma(4),
        ],
        compiler_params=pltpu.CompilerParams(
            collective_id=0, has_side_effects=True, vmem_limit_bytes=48 * 1024 * 1024
        ),
        name="layer",
    )(
        lambdas, queries[0], keys[0], values[0], value_gain.reshape(1, 128),
        jnp.asarray(inner), jnp.asarray(outer), out_weight.T,
    )
    return out[None]


def solution(mesh):
    return jax.shard_map(
        shards,
        mesh=mesh,
        in_specs=(
            P("dp", "sp", None),
            P("dp", "sp", None),
            P("dp", "sp", None),
            P(),
            P(),
            P(None, ("sp", "dp")),
        ),
        out_specs=P("dp", "sp", None),
        check_vma=False,
    )
```

```python
import functools

import jax
import jax.numpy as jnp
import numpy as np
from jax import lax
from jax.experimental import pallas as pl
from jax.experimental.pallas import tpu as pltpu
from jax.sharding import PartitionSpec as P

HEADS = 16
KV_HEADS = 4
HEAD_DIM = 64
VALUE_DIM = 128
D = 4096
SEQLEN = 2048
ROWS = 128
GROUP = HEADS // KV_HEADS
KT = 512
ROPE_BASE = 500000.0
OUTPUT_SCALE = 0.8
NORM_EPS = 1e-05
MESH = pl.DeviceIdType.MESH

COLOURS = ((0, 1024), (1024, 512), (1536, 512))


def rotation_tables():
    f32 = np.float32
    freqs = (f32(ROPE_BASE) ** (-np.arange(0, HEAD_DIM, 2, dtype=f32) / f32(HEAD_DIM))).astype(f32)
    lanes = np.tile(freqs.astype(np.float64), 4)
    inner = np.arange(ROWS)[:, None] * lanes[None]
    outer = (np.arange(SEQLEN // ROWS) * ROWS)[:, None] * lanes[None]
    inner = np.stack([np.cos(inner), np.sin(inner)]).astype(f32)
    outer = np.stack([np.cos(outer), np.sin(outer)], 1).astype(f32)
    return inner, outer


def kernel(
    lam_hbm, q_hbm, k_hbm, v_hbm, gain_hbm, inner_hbm, outer_hbm, w_hbm,
    out_ref,
    lam_ref, gain_ref, inner_ref, outer_ref, q_in, k_in, v_in,
    kvst, kv, qst, qin, q2, sbuf, acc, wbuf, hst, acts, pacc, oown, opart, oin,
    in_sem, sent, kvz_r, kvy_r, q_r, ring_r, fin_r, oz_r, af_r, oo_r,
):
    f32, bf16 = jnp.float32, jnp.bfloat16
    sp, dp = lax.axis_index("sp"), lax.axis_index("dp")
    me = {"z": sp // 4, "y": lax.rem(sp, 4), "x": dp // 2}
    core = lax.rem(dp, 2)

    def at(pos):
        return (pos["z"] * 4 + pos["y"], pos["x"] * 2 + core)

    def shift(dim, off):
        return {**me, dim: lax.rem(me[dim] + off + 4, 4)}

    partner = (sp, me["x"] * 2 + 1 - core)
    total_sent = [0, 0]

    def size(ref):
        return int(np.prod(ref.shape)) * ref.dtype.itemsize

    def amount(nbytes):
        rows = nbytes // 4096
        n = 1 if rows <= KT else (2 if rows % 16 == 0 and rows <= 2 * KT else 4)
        assert rows * 4096 == nbytes and rows % n == 0
        return sbuf.at[pl.ds(0, n), pl.ds(0, rows // n), :]

    def send(src, dst, r_sem, dev, kind=0):
        total_sent[kind] += size(src)
        pltpu.make_async_remote_copy(
            src_ref=src, dst_ref=dst, send_sem=sent.at[kind], recv_sem=r_sem, device_id=dev, device_id_type=MESH
        ).start()

    def arrived(nbytes, r_sem, name="wait"):
        view = amount(nbytes)
        with jax.named_scope(name):
            pltpu.make_async_remote_copy(
                src_ref=view, dst_ref=view, send_sem=sent.at[0], recv_sem=r_sem, device_id=partner, device_id_type=MESH
            ).wait_recv()

    barrier = pltpu.get_barrier_semaphore()
    peers = [at(shift("z", o)) for o in (1, 2, 3)] + [at(shift("y", o)) for o in (1, 3)]
    peers += [at(shift("x", o)) for o in (1, 3)] + [partner]
    for dev in peers:
        pl.semaphore_signal(barrier, inc=1, device_id=dev, device_id_type=MESH)

    copies = [
        pltpu.make_async_copy(src, dst, in_sem.at[n])
        for n, (src, dst) in enumerate((
            (k_hbm, k_in),
            (inner_hbm, inner_ref),
            (outer_hbm.at[sp], outer_ref),
            (v_hbm, v_in),
            (w_hbm, wbuf.at[me["z"], me["y"], me["x"]]),
            (q_hbm, q_in),
            (gain_hbm, gain_ref),
            (lam_hbm, lam_ref),
        ))
    ]
    for c in copies:
        c.start()
    c_k, c_in, c_out, c_v, c_w, c_q, c_gain, c_lam = copies
    c_in.wait()
    c_out.wait()

    ci, si = inner_ref[0], inner_ref[1]
    co, so = outer_ref[0:1, :], outer_ref[1:2, :]
    cosine = co * ci - so * si
    sine = so * ci + co * si
    row = lax.broadcasted_iota(jnp.int32, (128, 128), 0)
    col = lax.broadcasted_iota(jnp.int32, (128, 128), 1)
    low = lax.rem(col, 64) < 32
    swap = jnp.where(
        low & (row == col + 32), -1.0, jnp.where(jnp.logical_not(low) & (row == col - 32), 1.0, 0.0)
    ).astype(bf16)

    def rotate(part):
        turned = jnp.dot(part, swap, preferred_element_type=f32)
        return (part.astype(f32) * cosine + turned * sine).astype(bf16)

    with jax.named_scope("rotk"):
        c_k.wait()
        c_v.wait()
        for g in range(KV_HEADS):
            cols = slice(g * 128, (g + 1) * 128)
            kvst[g, 0] = rotate(k_in[:, cols])
            kvst[g, 1] = v_in[:, cols].astype(f32).T.astype(bf16)
    kv[sp, 0] = kvst[me["z"], 0]
    kv[sp, 1] = kvst[me["z"], 1]
    with jax.named_scope("barrier"):
        pl.semaphore_wait(barrier, len(peers))

    steps = (0, 3, 1, 2)
    block_bytes = size(kv.at[0])

    def kv_block(rel, off):
        return lax.rem(me["z"] + rel, 4) * 4 + lax.rem(me["y"] + off + 4, 4)

    def kvz_start(o):
        pos = shift("z", o)
        send(kvst.at[pos["z"]], kv.at[sp], kvz_r.at[o - 1], at(pos))

    def kvz_wait(rel):
        arrived(block_bytes, kvz_r.at[3 - rel], f"kvz_{rel}")

    def kvy_start(rel):
        view = kvst.at[me["z"]] if rel == 0 else kv.at[kv_block(rel, 0)]
        for off in (1, -1):
            send(view, kv.at[kv_block(rel, 0)], kvy_r.at[rel], at(shift("y", off)))

    def kvy_forward(rel):
        arrived(2 * block_bytes, kvy_r.at[rel], f"kvy_{rel}")
        for n, off in enumerate((-1, 1)):
            half = kv.at[kv_block(rel, off), n]
            send(half, half, kvy_r.at[4], at(shift("y", -off)))

    made = []

    class Ring:
        def __init__(self, colour, dim, fin, **fixed):
            self.dim, self.fixed = dim, fixed
            self.k0, self.kn = COLOURS[colour]
            self.full, self.fin = ring_r.at[len(made)], fin_r.at[fin]
            self.bytes = size(self.view(0))
            self.name = f"{len(made)}{dim}"
            made.append(self)

        def view(self, off, half=None):
            sel, rows = {}, slice(None)
            for d in "zyx":
                rel = off if d == self.dim else self.fixed[d]
                sel[d] = slice(None) if rel is None else lax.rem(me[d] + rel + 4, 4)
            if half is not None:
                free = [d for d in "zyx" if d != self.dim and self.fixed[d] is None]
                if free:
                    sel[free[0]] = pl.ds(2 * half, 2)
                else:
                    rows = pl.ds(16 * half, 16)
            return wbuf.at[sel["z"], sel["y"], sel["x"], rows, pl.ds(self.k0, self.kn)]

        def start(self):
            view = self.view(0)
            for off in (1, -1):
                send(view, view, self.full, at(shift(self.dim, off)), 1)

        def forward(self):
            arrived(2 * self.bytes, self.full, "fwd" + self.name)
            for n, off in enumerate((-1, 1)):
                half = self.view(off, n)
                send(half, half, self.fin, at(shift(self.dim, -off)), 1)

        def finish(self):
            arrived(self.bytes, self.fin, "fin" + self.name)

    x1 = Ring(0, "z", 0, y=0, x=0)
    x2 = {a: Ring(0, "y", 1 + a, z=a, x=0) for a in steps}
    x3 = {(a, b): Ring(0, "x", 5 + b, z=a, y=b) for b in steps for a in steps}
    y1 = Ring(1, "x", 9, z=0, y=0)
    y2 = Ring(1, "z", 10, x=None, y=0)
    y3 = {a: Ring(1, "y", 11 + a, x=None, z=a) for a in steps}
    z1 = Ring(2, "x", 15, z=0, y=0)
    z2 = Ring(2, "y", 16, x=None, z=0)
    z3 = {b: Ring(2, "z", 17 + b, x=None, y=b) for b in steps}

    def x3_finish(b):
        arrived(4 * x3[0, b].bytes, x3[0, b].fin, f"finx{b}")

    c_w.wait()
    for ring in (x1, x2[0], x3[0, 0], y1, z1):
        ring.start()
    for o in (1, 3, 2):
        kvz_start(o)
    kvy_start(0)

    with jax.named_scope("rotq"):
        c_q.wait()
        for g in range(KV_HEADS):
            for h in range(GROUP):
                a = (g * GROUP + h) * 128
                qst[g, :, h * 128:(h + 1) * 128] = rotate(q_in[:, a:a + 128])
    qin[me["z"]] = qst[me["z"]]
    x1.forward()
    for ring in (x3[3, 0], x3[1, 0]):
        ring.start()
    kvz_wait(3)
    kvy_start(3)
    kvz_wait(1)
    kvy_start(1)
    for o in (1, 3, 2):
        pos = shift("z", o)
        send(qst.at[pos["z"]], qin.at[me["z"]], q_r.at[o - 1], at(pos))
    x2[0].forward()
    for ring in (x3[0, 3], x3[0, 1]):
        ring.start()
    y1.forward()
    z1.forward()
    kvy_forward(0)
    for ring in (x2[3], x2[1]):
        ring.start()
    x3[0, 0].forward()
    x1.finish()
    x3[2, 0].start()
    kvz_wait(2)
    kvy_start(2)
    x2[2].start()
    y1.finish()
    z1.finish()
    y2.start()
    z3[0].start()
    kvy_forward(3)
    kvy_forward(1)
    x2[0].finish()
    x3[0, 2].start()
    x3[3, 0].forward()
    x3[1, 0].forward()
    for a in (3, 1):
        x2[a].forward()
        x3[a, 3].start()
        x3[a, 1].start()
    kvy_forward(2)
    pacc[...] = jnp.zeros_like(pacc)
    z2.start()
    y3[0].start()
    x3[0, 3].forward()
    x3[0, 1].forward()
    arrived(4 * block_bytes, kvy_r.at[4], "kvyf")

    scale = float(HEAD_DIM ** -0.5 * np.log2(np.e))
    c_lam.wait()
    lam = jnp.concatenate(
        [jnp.full((1, 128), lam_ref[me["z"] * GROUP + h], f32) for h in range(GROUP)], 1
    )
    lane = lax.broadcasted_iota(jnp.int32, (128, 128), 1)
    half_rows = GROUP * ROWS

    def attend(i, after):
        zq = lax.rem(me["z"] + 1 + i, 4)
        if i < 3:
            o = 3 - i
            arrived(size(qin.at[0]), q_r.at[o - 1], f"q_{i}")
        for m in range(2):
            keep = (lane < 64) if m == 0 else (lane >= 64)
            for h in range(GROUP):
                part = qin[zq, :, h * 128:(h + 1) * 128]
                q2[(m * GROUP + h) * 128:(m * GROUP + h + 1) * 128, :] = jnp.where(
                    keep, part, jnp.zeros_like(part)
                )
        block = zq * 4 + me["y"]
        last = zq

        def scores(t):
            keys = jnp.concatenate([kv[4 * t + b, 0] for b in range(4)], 0)
            return lax.dot_general(keys, q2[...], (((1,), (1,)), ((), ())), preferred_element_type=f32)

        def fold(x, op):
            r = x.reshape(KT // 8, 8, x.shape[1])
            return op(r, 0)

        def pass1(t, top):
            s = scores(t)
            sbuf[t] = s
            return jnp.maximum(top, fold(s, jnp.max))

        scope = jax.named_scope(f"pass1_{i}")
        scope.__enter__()
        top = lax.fori_loop(0, last, pass1, jnp.full((8, 2 * half_rows), -1e30, f32))
        s = scores(last)
        key_at = lax.broadcasted_iota(jnp.int32, (KT, 2 * half_rows), 0) + last * KT
        query_at = lax.rem(lax.broadcasted_iota(jnp.int32, (KT, 2 * half_rows), 1), 128) + block * 128
        s = jnp.where(key_at <= query_at, s, -1e30)
        sbuf[last] = s
        top = jnp.maximum(top, fold(s, jnp.max))
        top = jnp.max(top, 0, keepdims=True)
        scope.__exit__(None, None, None)
        after[0]()

        def pass2(t, total):
            p = jnp.exp2((sbuf[t] - top) * scale)
            sbuf[t] = p
            return total + fold(p, jnp.sum)

        with jax.named_scope(f"pass2_{i}"):
            total = lax.fori_loop(0, last + 1, pass2, jnp.zeros((8, 2 * half_rows), f32))
        after[1]()
        total = jnp.sum(total, 0, keepdims=True)
        a0 = 1.0 / total[:, :half_rows]
        a1 = lam / total[:, half_rows:]
        acc[...] = jnp.zeros_like(acc)

        def pass3(t, carry):
            w = (sbuf[t, :, :half_rows] * a0 - sbuf[t, :, half_rows:] * a1).astype(bf16)
            vals = jnp.concatenate([kv[4 * t + b, 1] for b in range(4)], 1)
            acc[...] += jnp.dot(vals, w, preferred_element_type=f32)
            return carry

        with jax.named_scope(f"pass3_{i}"):
            lax.fori_loop(0, last + 1, pass3, 0)
        after[2]()
        hv = acc[...]
        inv = lax.rsqrt(jnp.mean(hv * hv, 0, keepdims=True) + NORM_EPS)
        hv = hv * inv
        for h in range(GROUP):
            piece = hv[:, h * 128:(h + 1) * 128].T
            hst[zq, :, h * 128:(h + 1) * 128] = (piece * gain_ref[...] * OUTPUT_SCALE).astype(bf16)
        return zq

    def ship(i, zq):
        if i < 3:
            o = i + 1
            send(hst.at[zq], acts.at[0, me["z"]], oz_r.at[o - 1], at(shift("z", o)))
        else:
            acts[0, me["z"]] = hst[me["z"]]
            send(hst.at[me["z"]], acts.at[1, me["z"]], af_r.at[0], partner)

    def acts_in(o):
        g = lax.rem(me["z"] + 4 - o, 4)
        arrived(size(acts.at[0, 0]), oz_r.at[o - 1], f"o_{o}")
        send(acts.at[0, g], acts.at[1, g], af_r.at[0], partner)

    def multiply(heads, weights):
        total = None
        for n, g in enumerate(heads):
            part = lax.dot_general(
                acts[:, g].reshape(2 * ROWS, 512), weights[:, n * 512:(n + 1) * 512],
                (((1,), (1,)), ((), ())), preferred_element_type=f32,
            )
            total = part if total is None else total + part
        return total

    def project_xz(b):
        with jax.named_scope(f"proj_xz{b}"):
            yb = lax.rem(me["y"] + b, 4)
            cat = lambda lo, hi: jnp.concatenate(
                [wbuf[z, yb, :, :, lo:hi].reshape(128, hi - lo) for z in range(4)], 0
            )
            part = multiply((0, 1), cat(0, 1024)) + multiply((3,), cat(1536, 2048))
            for z in range(4):
                pacc[z, yb] += part[:, z * 128:(z + 1) * 128]

    def project_y(a):
        with jax.named_scope(f"proj_y{a}"):
            za = lax.rem(me["z"] + a, 4)
            part = multiply((2,), wbuf[za, :, :, :, 1024:1536].reshape(512, 512))
            for y in range(4):
                pacc[za, y] += part[:, y * 128:(y + 1) * 128]

    early = [(a, b) for a in (0, 3, 1) for b in (0, 3, 1)]
    late = [(2, b) for b in (0, 3, 1)] + [(a, 2) for a in steps]

    def tile_of(a, b):
        return lax.rem(me["z"] + a, 4), lax.rem(me["y"] + b, 4)

    def swap_tiles(tiles, n):
        for a, b in tiles:
            z, y = tile_of(a, b)
            opart[z, y] = pacc[z, y, ROWS:].astype(bf16)
        for a, b in tiles:
            z, y = tile_of(a, b)
            send(opart.at[z, y], oin.at[z, y], oo_r.at[n], partner)
            oown[z, y] = pacc[z, y, :ROWS].astype(bf16)

    erow = lax.broadcasted_iota(jnp.int32, (256, 256), 0)
    ecol = lax.broadcasted_iota(jnp.int32, (256, 256), 1)
    mine = jnp.where(erow < 128, core, 1 - core)
    er = lax.rem(erow, 128)
    spread = jnp.where(ecol == (er // 32) * 64 + mine * 32 + lax.rem(er, 32), 1.0, 0.0).astype(bf16)

    def merge(tiles, n):
        arrived(len(tiles) * size(oin.at[0, 0]), oo_r.at[n], f"swap_{n}")
        with jax.named_scope(f"merge_{n}"):
            for a, b in tiles:
                z, y = tile_of(a, b)
                both = jnp.concatenate([oown[z, y], oin[z, y]], 1)
                cols = pl.ds(pl.multiple_of((z * 4 + y) * 256, 256), 256)
                out_ref[:, cols] = jnp.dot(both, spread, preferred_element_type=f32).astype(bf16)

    def nothing():
        pass

    def h00():
        x2[2].forward()
        x3[2, 3].start()
        x3[2, 1].start()

    def h01():
        for a in (3, 1):
            x2[a].finish()
            x3[a, 2].start()
        x3[2, 0].forward()

    def h10():
        y2.forward()
        y3[3].start()
        y3[1].start()
        x3[0, 2].forward()

    def h11():
        x2[2].finish()
        x3[2, 2].start()
        z2.forward()
        z3[3].start()
        z3[1].start()

    def h12():
        x3[3, 3].forward()

    def h20():
        x3[3, 1].forward()
        z3[0].forward()

    def h21():
        y2.finish()
        y3[2].start()

    def h22():
        z2.finish()
        z3[2].start()
        y3[0].forward()
        x3[1, 3].forward()

    def h30():
        x3[1, 1].forward()
        x3[2, 3].forward()

    c_gain.wait()
    hooks = ((h00, h01, nothing), (h10, h11, h12), (h20, h21, h22), (h30, nothing, nothing))
    for i in range(4):
        ship(i, attend(i, hooks[i]))
    acts_in(1)
    x3[2, 1].forward()
    acts_in(2)
    acts_in(3)
    z3[3].forward()
    y3[3].forward()
    x3_finish(0)
    z3[0].finish()
    x3[3, 2].forward()
    arrived(4 * size(acts.at[0, 0]), af_r.at[0], "acts")
    project_xz(0)
    z3[1].forward()
    y3[1].forward()
    x3[1, 2].forward()
    y3[0].finish()
    project_y(0)
    x3[2, 2].forward()
    x3_finish(3)
    z3[3].finish()
    project_xz(3)
    z3[2].forward()
    y3[2].forward()
    y3[3].finish()
    project_y(3)
    x3_finish(1)
    z3[1].finish()
    project_xz(1)
    y3[1].finish()
    project_y(1)
    swap_tiles(early, 0)
    x3_finish(2)
    z3[2].finish()
    project_xz(2)
    y3[2].finish()
    project_y(2)
    swap_tiles(late, 1)
    merge(early, 0)
    merge(late, 1)
    with jax.named_scope("drain"):
        for kind in (0, 1):
            view = amount(total_sent[kind])
            pltpu.make_async_remote_copy(
                src_ref=view, dst_ref=view, send_sem=sent.at[kind], recv_sem=oo_r.at[0],
                device_id=partner, device_id_type=MESH,
            ).wait_send()


def shards(queries, keys, values, lambdas, value_gain, out_weight):
    inner, outer = rotation_tables()
    vmem = pl.BlockSpec(memory_space=pltpu.VMEM)
    hbm = pl.BlockSpec(memory_space=pltpu.HBM)
    bf16, f32 = jnp.bfloat16, jnp.float32
    dma = lambda n: pltpu.SemaphoreType.DMA((n,))
    out = pl.pallas_call(
        kernel,
        out_shape=jax.ShapeDtypeStruct((ROWS, D), bf16),
        in_specs=[hbm] * 8,
        out_specs=vmem,
        scratch_shapes=[
            pltpu.SMEM((HEADS,), f32),
            pltpu.VMEM((1, 128), f32),
            pltpu.VMEM((2, ROWS, 128), f32),
            pltpu.VMEM((2, 128), f32),
            pltpu.VMEM((ROWS, 2048), bf16),
            pltpu.VMEM((ROWS, 512), bf16),
            pltpu.VMEM((ROWS, 512), bf16),
            pltpu.VMEM((4, 2, 128, 128), bf16),
            pltpu.VMEM((16, 2, 128, 128), bf16),
            pltpu.VMEM((4, 128, 512), bf16),
            pltpu.VMEM((4, 128, 512), bf16),
            pltpu.VMEM((1024, 128), bf16),
            pltpu.VMEM((SEQLEN // KT, KT, 1024), f32),
            pltpu.VMEM((128, 512), f32),
            pltpu.VMEM((4, 4, 4, 32, 2048), bf16),
            pltpu.VMEM((4, 128, 512), bf16),
            pltpu.VMEM((2, 4, 128, 512), bf16),
            pltpu.VMEM((4, 4, 256, 128), f32),
            pltpu.VMEM((4, 4, 128, 128), bf16),
            pltpu.VMEM((4, 4, 128, 128), bf16),
            pltpu.VMEM((4, 4, 128, 128), bf16),
            dma(8), dma(2), dma(3), dma(5), dma(3), dma(33), dma(21), dma(3), dma(1), dma(2),
        ],
        compiler_params=pltpu.CompilerParams(
            collective_id=0, has_side_effects=True, vmem_limit_bytes=50_000_000
        ),
        name="layer",
    )(*(
        pltpu.with_memory_space_constraint(a, pltpu.HBM)
        for a in (
            lambdas, queries[0], keys[0], values[0], value_gain.reshape(1, 128),
            jnp.asarray(inner), jnp.asarray(outer), out_weight.T,
        )
    ))
    return out[None]


def solution(mesh):
    return jax.shard_map(
        shards,
        mesh=mesh,
        in_specs=(
            P("dp", "sp", None),
            P("dp", "sp", None),
            P("dp", "sp", None),
            P(),
            P(),
            P(None, ("sp", "dp")),
        ),
        out_specs=P("dp", "sp", None),
        check_vma=False,
    )
```

```python
import functools

import jax
import jax.numpy as jnp
import numpy as np
from jax import lax
from jax.experimental import pallas as pl
from jax.experimental.pallas import tpu as pltpu
from jax.sharding import PartitionSpec as P

HEADS = 16
KV_HEADS = 4
HEAD_DIM = 64
VALUE_DIM = 128
D = 4096
SEQLEN = 2048
ROWS = 128
GROUP = HEADS // KV_HEADS
KT = 512
ROPE_BASE = 500000.0
OUTPUT_SCALE = 0.8
NORM_EPS = 1e-05
MESH = pl.DeviceIdType.MESH

COLOURS = ((0, 1024), (1024, 512), (1536, 512))

ORDER = (
    "kvy0s", "x300s", "z1s", "kvzs", "y1s", "x1s", "x20s", "rotq", "qs", "kvy0f", "x300f", "kvz3w", "kvy3s",
    "kvz1w", "kvy1s", "z1f", "x20f", "x301s", "x303s", "y1f", "kvz2w", "kvy2s", "x1f", "x310s", "x330s",
    "z1e", "z2s", "x21s", "z30s", "x23s", "kvy3f", "x301f", "kvy1f", "x20e", "x303f", "x302s", "y1e", "y2s",
    "y30s", "kvy2f", "x310f", "x1e", "x320s", "x22s", "x330f", "z2f", "z33s", "z31s", "x21f", "x311s",
    "x313s", "z30f", "x302f", "x23f", "x333s", "x331s", "x320f", "y2f", "y33s", "y31s", "x311f", "y30f",
    "z33f", "x313f", "kvall", "at00", "at01", "x333f", "x22f", "x321s", "x323s", "at02", "z2e", "z32s",
    "at10", "x21e", "x312s", "x23e", "x332s", "x331f", "at11", "at12", "y2e", "y32s", "at20", "at21", "x321f",
    "at22", "x323f", "at30", "at31", "x312f", "at32", "x332f", "y30e", "z31f", "y31f", "y33f", "z33e", "o1w",
    "x22e", "x322s", "z30e", "z32f", "y32f", "o3w", "o2w", "y31e", "z31e", "x322f", "acts", "py0", "pxz3",
    "pxz1", "y33e", "py3", "py1", "pxz0", "sw0", "z32e", "y32e", "py2", "pxz2", "sw1", "m0", "m1",
)


def rotation_tables():
    f32 = np.float32
    freqs = (f32(ROPE_BASE) ** (-np.arange(0, HEAD_DIM, 2, dtype=f32) / f32(HEAD_DIM))).astype(f32)
    lanes = np.tile(freqs.astype(np.float64), 4)
    inner = np.arange(ROWS)[:, None] * lanes[None]
    outer = (np.arange(SEQLEN // ROWS) * ROWS)[:, None] * lanes[None]
    inner = np.stack([np.cos(inner), np.sin(inner)]).astype(f32)
    outer = np.stack([np.cos(outer), np.sin(outer)], 1).astype(f32)
    return inner, outer


def kernel(
    lam_hbm, q_hbm, k_hbm, v_hbm, gain_hbm, inner_hbm, outer_hbm, w_hbm,
    out_ref,
    lam_ref, gain_ref, inner_ref, outer_ref, q_in, k_in, v_in,
    kvst, kv, qst, qin, q2, sbuf, acc, wbuf, hst, acts, pacc, oown, opart, oin,
    in_sem, sent, kvz_r, kvy_r, q_r, ring_r, fin_r, oz_r, af_r, oo_r,
):
    f32, bf16 = jnp.float32, jnp.bfloat16
    sp, dp = lax.axis_index("sp"), lax.axis_index("dp")
    me = {"z": sp // 4, "y": lax.rem(sp, 4), "x": dp // 2}
    core = lax.rem(dp, 2)

    def at(pos):
        return (pos["z"] * 4 + pos["y"], pos["x"] * 2 + core)

    def shift(dim, off):
        return {**me, dim: lax.rem(me[dim] + off + 4, 4)}

    partner = (sp, me["x"] * 2 + 1 - core)
    total_sent = [0, 0]

    def size(ref):
        return int(np.prod(ref.shape)) * ref.dtype.itemsize

    def amount(nbytes):
        rows = nbytes // 4096
        n = 1 if rows <= KT else (2 if rows % 16 == 0 and rows <= 2 * KT else 4)
        assert rows * 4096 == nbytes and rows % n == 0
        return sbuf.at[pl.ds(0, n), pl.ds(0, rows // n), :]

    def send(src, dst, r_sem, dev, kind=0):
        total_sent[kind] += size(src)
        pltpu.make_async_remote_copy(
            src_ref=src, dst_ref=dst, send_sem=sent.at[kind], recv_sem=r_sem, device_id=dev, device_id_type=MESH
        ).start()

    def arrived(nbytes, r_sem, name="wait"):
        view = amount(nbytes)
        with jax.named_scope(name):
            pltpu.make_async_remote_copy(
                src_ref=view, dst_ref=view, send_sem=sent.at[0], recv_sem=r_sem, device_id=partner, device_id_type=MESH
            ).wait_recv()

    barrier = pltpu.get_barrier_semaphore()
    peers = [at(shift("z", o)) for o in (1, 2, 3)] + [at(shift("y", o)) for o in (1, 3)]
    peers += [at(shift("x", o)) for o in (1, 3)] + [partner]
    for dev in peers:
        pl.semaphore_signal(barrier, inc=1, device_id=dev, device_id_type=MESH)

    copies = [
        pltpu.make_async_copy(src, dst, in_sem.at[n])
        for n, (src, dst) in enumerate((
            (k_hbm, k_in),
            (inner_hbm, inner_ref),
            (outer_hbm.at[sp], outer_ref),
            (v_hbm, v_in),
            (w_hbm, wbuf.at[me["z"], me["y"], me["x"]]),
            (q_hbm, q_in),
            (gain_hbm, gain_ref),
            (lam_hbm, lam_ref),
        ))
    ]
    for c in copies:
        c.start()
    c_k, c_in, c_out, c_v, c_w, c_q, c_gain, c_lam = copies
    c_in.wait()
    c_out.wait()

    ci, si = inner_ref[0], inner_ref[1]
    co, so = outer_ref[0:1, :], outer_ref[1:2, :]
    cosine = co * ci - so * si
    sine = so * ci + co * si
    row = lax.broadcasted_iota(jnp.int32, (128, 128), 0)
    col = lax.broadcasted_iota(jnp.int32, (128, 128), 1)
    low = lax.rem(col, 64) < 32
    swap = jnp.where(
        low & (row == col + 32), -1.0, jnp.where(jnp.logical_not(low) & (row == col - 32), 1.0, 0.0)
    ).astype(bf16)

    def rotate(part):
        turned = jnp.dot(part, swap, preferred_element_type=f32)
        return (part.astype(f32) * cosine + turned * sine).astype(bf16)

    with jax.named_scope("rotk"):
        c_k.wait()
        c_v.wait()
        for g in range(KV_HEADS):
            cols = slice(g * 128, (g + 1) * 128)
            kvst[g, 0] = rotate(k_in[:, cols])
            kvst[g, 1] = v_in[:, cols].astype(f32).T.astype(bf16)
    kv[sp, 0] = kvst[me["z"], 0]
    kv[sp, 1] = kvst[me["z"], 1]
    with jax.named_scope("barrier"):
        pl.semaphore_wait(barrier, len(peers))

    steps = (0, 3, 1, 2)
    block_bytes = size(kv.at[0])

    def kv_block(rel, off):
        return lax.rem(me["z"] + rel, 4) * 4 + lax.rem(me["y"] + off + 4, 4)

    def kvz_start(o):
        pos = shift("z", o)
        send(kvst.at[pos["z"]], kv.at[sp], kvz_r.at[o - 1], at(pos))

    def kvz_wait(rel):
        arrived(block_bytes, kvz_r.at[3 - rel], f"kvz_{rel}")

    def kvy_start(rel):
        view = kvst.at[me["z"]] if rel == 0 else kv.at[kv_block(rel, 0)]
        for off in (1, -1):
            send(view, kv.at[kv_block(rel, 0)], kvy_r.at[rel], at(shift("y", off)))

    def kvy_forward(rel):
        arrived(2 * block_bytes, kvy_r.at[rel], f"kvy_{rel}")
        for n, off in enumerate((-1, 1)):
            half = kv.at[kv_block(rel, off), n]
            send(half, half, kvy_r.at[4], at(shift("y", -off)))

    made = []

    class Ring:
        def __init__(self, colour, dim, fin, **fixed):
            self.dim, self.fixed = dim, fixed
            self.k0, self.kn = COLOURS[colour]
            self.full, self.fin = ring_r.at[len(made)], fin_r.at[fin]
            self.bytes = size(self.view(0))
            self.name = f"{len(made)}{dim}"
            made.append(self)

        def view(self, off, half=None):
            sel, rows = {}, slice(None)
            for d in "zyx":
                rel = off if d == self.dim else self.fixed[d]
                sel[d] = slice(None) if rel is None else lax.rem(me[d] + rel + 4, 4)
            if half is not None:
                free = [d for d in "zyx" if d != self.dim and self.fixed[d] is None]
                if free:
                    sel[free[0]] = pl.ds(2 * half, 2)
                else:
                    rows = pl.ds(16 * half, 16)
            return wbuf.at[sel["z"], sel["y"], sel["x"], rows, pl.ds(self.k0, self.kn)]

        def start(self):
            view = self.view(0)
            for off in (1, -1):
                send(view, view, self.full, at(shift(self.dim, off)), 1)

        def forward(self):
            arrived(2 * self.bytes, self.full, "fwd" + self.name)
            for n, off in enumerate((-1, 1)):
                half = self.view(off, n)
                send(half, half, self.fin, at(shift(self.dim, -off)), 1)

        def finish(self):
            arrived(self.bytes, self.fin, "fin" + self.name)

    x1 = Ring(0, "z", 0, y=0, x=0)
    x2 = {a: Ring(0, "y", 1 + a, z=a, x=0) for a in steps}
    x3 = {(a, b): Ring(0, "x", 5 + b, z=a, y=b) for b in steps for a in steps}
    y1 = Ring(1, "x", 9, z=0, y=0)
    y2 = Ring(1, "z", 10, x=None, y=0)
    y3 = {a: Ring(1, "y", 11 + a, x=None, z=a) for a in steps}
    z1 = Ring(2, "x", 15, z=0, y=0)
    z2 = Ring(2, "y", 16, x=None, z=0)
    z3 = {b: Ring(2, "z", 17 + b, x=None, y=b) for b in steps}

    def x3_finish(b):
        arrived(4 * x3[0, b].bytes, x3[0, b].fin, f"finx{b}")

    c_w.wait()
    tasks = {"kvzs": lambda: [kvz_start(o) for o in (1, 3, 2)]}
    for a in steps:
        tasks[f"kvz{a}w"] = functools.partial(kvz_wait, a)
        tasks[f"kvy{a}s"] = functools.partial(kvy_start, a)
        tasks[f"kvy{a}f"] = functools.partial(kvy_forward, a)
    tasks["kvall"] = lambda: arrived(4 * block_bytes, kvy_r.at[4], "kvyf")
    rings = {"x1": x1, "y1": y1, "z1": z1, "y2": y2, "z2": z2}
    for a in steps:
        rings.update({f"x2{a}": x2[a], f"y3{a}": y3[a], f"z3{a}": z3[a]})
        rings.update({f"x3{a}{b}": x3[a, b] for b in steps})
    for name, ring in rings.items():
        tasks.update({name + "s": ring.start, name + "f": ring.forward, name + "e": ring.finish})

    def rotate_queries():
        with jax.named_scope("rotq"):
            c_q.wait()
            for g in range(KV_HEADS):
                for h in range(GROUP):
                    a = (g * GROUP + h) * 128
                    qst[g, :, h * 128:(h + 1) * 128] = rotate(q_in[:, a:a + 128])
            qin[me["z"]] = qst[me["z"]]
            pacc[...] = jnp.zeros_like(pacc)

    def send_queries():
        for o in (1, 3, 2):
            pos = shift("z", o)
            send(qst.at[pos["z"]], qin.at[me["z"]], q_r.at[o - 1], at(pos))

    tasks.update({"rotq": rotate_queries, "qs": send_queries})

    scale = float(HEAD_DIM ** -0.5 * np.log2(np.e))
    c_lam.wait()
    lam = jnp.concatenate(
        [jnp.full((1, 128), lam_ref[me["z"] * GROUP + h], f32) for h in range(GROUP)], 1
    )
    lane = lax.broadcasted_iota(jnp.int32, (128, 128), 1)
    half_rows = GROUP * ROWS

    kept = {}

    def fold(x, op):
        return op(x.reshape(KT // 8, 8, x.shape[1]), 0)

    def attend_scores(i):
        zq = lax.rem(me["z"] + 1 + i, 4)
        if i < 3:
            o = 3 - i
            arrived(size(qin.at[0]), q_r.at[o - 1], f"q_{i}")
        for m in range(2):
            keep = (lane < 64) if m == 0 else (lane >= 64)
            for h in range(GROUP):
                part = qin[zq, :, h * 128:(h + 1) * 128]
                q2[(m * GROUP + h) * 128:(m * GROUP + h + 1) * 128, :] = jnp.where(
                    keep, part, jnp.zeros_like(part)
                )
        block = zq * 4 + me["y"]
        last = zq

        def scores(t):
            keys = jnp.concatenate([kv[4 * t + b, 0] for b in range(4)], 0)
            return lax.dot_general(keys, q2[...], (((1,), (1,)), ((), ())), preferred_element_type=f32)

        def pass1(t, top):
            s = scores(t)
            sbuf[t] = s
            return jnp.maximum(top, fold(s, jnp.max))

        top = lax.fori_loop(0, last, pass1, jnp.full((8, 2 * half_rows), -1e30, f32))
        s = scores(last)
        key_at = lax.broadcasted_iota(jnp.int32, (KT, 2 * half_rows), 0) + last * KT
        query_at = lax.rem(lax.broadcasted_iota(jnp.int32, (KT, 2 * half_rows), 1), 128) + block * 128
        s = jnp.where(key_at <= query_at, s, -1e30)
        sbuf[last] = s
        top = jnp.maximum(top, fold(s, jnp.max))
        top = jnp.max(top, 0, keepdims=True)
        kept["top"] = top

    def attend_exp(i):
        last = lax.rem(me["z"] + 1 + i, 4)
        top = kept["top"]

        def pass2(t, total):
            p = jnp.exp2((sbuf[t] - top) * scale)
            sbuf[t] = p
            return total + fold(p, jnp.sum)

        total = lax.fori_loop(0, last + 1, pass2, jnp.zeros((8, 2 * half_rows), f32))
        kept["total"] = jnp.sum(total, 0, keepdims=True)

    def attend_values(i):
        zq = last = lax.rem(me["z"] + 1 + i, 4)
        total = kept["total"]
        a0 = 1.0 / total[:, :half_rows]
        a1 = lam / total[:, half_rows:]
        acc[...] = jnp.zeros_like(acc)

        def pass3(t, carry):
            w = (sbuf[t, :, :half_rows] * a0 - sbuf[t, :, half_rows:] * a1).astype(bf16)
            vals = jnp.concatenate([kv[4 * t + b, 1] for b in range(4)], 1)
            acc[...] += jnp.dot(vals, w, preferred_element_type=f32)
            return carry

        lax.fori_loop(0, last + 1, pass3, 0)
        hv = acc[...]
        inv = lax.rsqrt(jnp.mean(hv * hv, 0, keepdims=True) + NORM_EPS)
        hv = hv * inv
        for h in range(GROUP):
            piece = hv[:, h * 128:(h + 1) * 128].T
            hst[zq, :, h * 128:(h + 1) * 128] = (piece * gain_ref[...] * OUTPUT_SCALE).astype(bf16)
        ship(i, zq)

    def ship(i, zq):
        if i < 3:
            o = i + 1
            send(hst.at[zq], acts.at[0, me["z"]], oz_r.at[o - 1], at(shift("z", o)))
        else:
            acts[0, me["z"]] = hst[me["z"]]
            send(hst.at[me["z"]], acts.at[1, me["z"]], af_r.at[0], partner)

    def acts_in(o):
        g = lax.rem(me["z"] + 4 - o, 4)
        arrived(size(acts.at[0, 0]), oz_r.at[o - 1], f"o_{o}")
        send(acts.at[0, g], acts.at[1, g], af_r.at[0], partner)

    def multiply(heads, weights):
        total = None
        for n, g in enumerate(heads):
            part = lax.dot_general(
                acts[:, g].reshape(2 * ROWS, 512), weights[:, n * 512:(n + 1) * 512],
                (((1,), (1,)), ((), ())), preferred_element_type=f32,
            )
            total = part if total is None else total + part
        return total

    def project_xz(b):
        with jax.named_scope(f"proj_xz{b}"):
            yb = lax.rem(me["y"] + b, 4)
            cat = lambda lo, hi: jnp.concatenate(
                [wbuf[z, yb, :, :, lo:hi].reshape(128, hi - lo) for z in range(4)], 0
            )
            part = multiply((0, 1), cat(0, 1024)) + multiply((3,), cat(1536, 2048))
            for z in range(4):
                pacc[z, yb] += part[:, z * 128:(z + 1) * 128]

    def project_y(a):
        with jax.named_scope(f"proj_y{a}"):
            za = lax.rem(me["z"] + a, 4)
            part = multiply((2,), wbuf[za, :, :, :, 1024:1536].reshape(512, 512))
            for y in range(4):
                pacc[za, y] += part[:, y * 128:(y + 1) * 128]

    early = [(a, b) for a in (0, 3, 1) for b in (0, 3, 1)]
    late = [(2, b) for b in (0, 3, 1)] + [(a, 2) for a in steps]

    def tile_of(a, b):
        return lax.rem(me["z"] + a, 4), lax.rem(me["y"] + b, 4)

    def swap_tiles(tiles, n):
        for a, b in tiles:
            z, y = tile_of(a, b)
            opart[z, y] = pacc[z, y, ROWS:].astype(bf16)
        for a, b in tiles:
            z, y = tile_of(a, b)
            send(opart.at[z, y], oin.at[z, y], oo_r.at[n], partner)
            oown[z, y] = pacc[z, y, :ROWS].astype(bf16)

    erow = lax.broadcasted_iota(jnp.int32, (256, 256), 0)
    ecol = lax.broadcasted_iota(jnp.int32, (256, 256), 1)
    mine = jnp.where(erow < 128, core, 1 - core)
    er = lax.rem(erow, 128)
    spread = jnp.where(ecol == (er // 32) * 64 + mine * 32 + lax.rem(er, 32), 1.0, 0.0).astype(bf16)

    def merge(tiles, n):
        arrived(len(tiles) * size(oin.at[0, 0]), oo_r.at[n], f"swap_{n}")
        with jax.named_scope(f"merge_{n}"):
            for a, b in tiles:
                z, y = tile_of(a, b)
                both = jnp.concatenate([oown[z, y], oin[z, y]], 1)
                cols = pl.ds(pl.multiple_of((z * 4 + y) * 256, 256), 256)
                out_ref[:, cols] = jnp.dot(both, spread, preferred_element_type=f32).astype(bf16)

    def scoped(name, fn, *args):
        with jax.named_scope(name):
            fn(*args)

    def project_xz_task(b):
        x3_finish(b)
        project_xz(b)

    for i in range(4):
        for n, fn in enumerate((attend_scores, attend_exp, attend_values)):
            tasks[f"at{i}{n}"] = functools.partial(scoped, f"at{i}{n}", fn, i)
    for o in (1, 2, 3):
        tasks[f"o{o}w"] = functools.partial(acts_in, o)
    tasks["acts"] = lambda: arrived(4 * size(acts.at[0, 0]), af_r.at[0], "acts")
    for b in steps:
        tasks[f"pxz{b}"] = functools.partial(project_xz_task, b)
        tasks[f"py{b}"] = functools.partial(project_y, b)
    tasks["sw0"] = functools.partial(swap_tiles, early, 0)
    tasks["sw1"] = functools.partial(swap_tiles, late, 1)
    tasks["m0"] = functools.partial(merge, early, 0)
    tasks["m1"] = functools.partial(merge, late, 1)
    c_gain.wait()
    left = [n for n in tasks if not (n.startswith("x3") and n.endswith("e"))]
    left.remove("kvz0w")
    assert sorted(left) == sorted(ORDER)
    for name in ORDER:
        tasks[name]()
    with jax.named_scope("drain"):
        for kind in (0, 1):
            view = amount(total_sent[kind])
            pltpu.make_async_remote_copy(
                src_ref=view, dst_ref=view, send_sem=sent.at[kind], recv_sem=oo_r.at[0],
                device_id=partner, device_id_type=MESH,
            ).wait_send()


def shards(queries, keys, values, lambdas, value_gain, out_weight):
    inner, outer = rotation_tables()
    vmem = pl.BlockSpec(memory_space=pltpu.VMEM)
    hbm = pl.BlockSpec(memory_space=pltpu.HBM)
    bf16, f32 = jnp.bfloat16, jnp.float32
    dma = lambda n: pltpu.SemaphoreType.DMA((n,))
    out = pl.pallas_call(
        kernel,
        out_shape=jax.ShapeDtypeStruct((ROWS, D), bf16),
        in_specs=[hbm] * 8,
        out_specs=vmem,
        scratch_shapes=[
            pltpu.SMEM((HEADS,), f32),
            pltpu.VMEM((1, 128), f32),
            pltpu.VMEM((2, ROWS, 128), f32),
            pltpu.VMEM((2, 128), f32),
            pltpu.VMEM((ROWS, 2048), bf16),
            pltpu.VMEM((ROWS, 512), bf16),
            pltpu.VMEM((ROWS, 512), bf16),
            pltpu.VMEM((4, 2, 128, 128), bf16),
            pltpu.VMEM((16, 2, 128, 128), bf16),
            pltpu.VMEM((4, 128, 512), bf16),
            pltpu.VMEM((4, 128, 512), bf16),
            pltpu.VMEM((1024, 128), bf16),
            pltpu.VMEM((SEQLEN // KT, KT, 1024), f32),
            pltpu.VMEM((128, 512), f32),
            pltpu.VMEM((4, 4, 4, 32, 2048), bf16),
            pltpu.VMEM((4, 128, 512), bf16),
            pltpu.VMEM((2, 4, 128, 512), bf16),
            pltpu.VMEM((4, 4, 256, 128), f32),
            pltpu.VMEM((4, 4, 128, 128), bf16),
            pltpu.VMEM((4, 4, 128, 128), bf16),
            pltpu.VMEM((4, 4, 128, 128), bf16),
            dma(8), dma(2), dma(3), dma(5), dma(3), dma(33), dma(21), dma(3), dma(1), dma(2),
        ],
        compiler_params=pltpu.CompilerParams(
            collective_id=0, has_side_effects=True, vmem_limit_bytes=50_000_000
        ),
        name="layer",
    )(*(
        pltpu.with_memory_space_constraint(a, pltpu.HBM)
        for a in (
            lambdas, queries[0], keys[0], values[0], value_gain.reshape(1, 128),
            jnp.asarray(inner), jnp.asarray(outer), out_weight.T,
        )
    ))
    return out[None]


def solution(mesh):
    return jax.shard_map(
        shards,
        mesh=mesh,
        in_specs=(
            P("dp", "sp", None),
            P("dp", "sp", None),
            P("dp", "sp", None),
            P(),
            P(),
            P(None, ("sp", "dp")),
        ),
        out_specs=P("dp", "sp", None),
        check_vma=False,
    )
```

```python
import functools

import jax
import jax.numpy as jnp
import numpy as np
from jax import lax
from jax.experimental import pallas as pl
from jax.experimental.pallas import tpu as pltpu
from jax.sharding import PartitionSpec as P

HEADS = 16
KV_HEADS = 4
HEAD_DIM = 64
VALUE_DIM = 128
D = 4096
SEQLEN = 2048
ROWS = 128
GROUP = HEADS // KV_HEADS
KT = 512
ROPE_BASE = 500000.0
OUTPUT_SCALE = 0.8
NORM_EPS = 1e-05
MESH = pl.DeviceIdType.MESH

COLOURS = ((0, 1024), (1024, 512), (1536, 512))

DIRECT = (2,)
ORDER = (
    "x20s", "z1s", "y1s", "x300s", "x1s", "rotk", "kvzs", "kvy0s", "rotq", "kvy0f", "qs", "z1f", "kvz1w",
    "kvy1s", "kvz3w", "kvy3s", "x20f", "x301s", "y1f", "x303s", "x1f", "x310s", "x330s", "x300f", "kvz2w",
    "kvy2s", "z1e", "z30s", "kvy1f", "z2s", "x21s", "x301f", "y1e", "y2s", "kvy3f", "x23s", "x303f", "x20e",
    "x302s", "x310f", "x1e", "x320s", "x22s", "x330f", "z30f", "x302f", "z2f", "z31s", "z33s", "x21f", "y2f",
    "y33s", "x313s", "x311s", "x320f", "kvall", "at00", "at01", "x23f", "x331s", "at02", "x22f", "x323s",
    "x321s", "y30s", "at10", "z2e", "z32s", "x313f", "at11", "x311f", "x21e", "x312s", "at12", "y31s", "at20",
    "x331f", "at21", "y2e", "y32s", "at22", "x323f", "x23e", "x332s", "at30", "x321f", "at31", "o1w", "at32",
    "y30f", "x333s", "z30e", "z31f", "x302e", "z33f", "y33f", "x22e", "x322s", "x312f", "z32f", "y31f",
    "x332f", "o3w", "o2w", "x333f", "z31e", "y32f", "acts", "pxz1", "z33e", "pxz0", "x312e", "x322f", "y30e",
    "py0", "y33e", "py3", "z32e", "pz2", "pxz3", "y31e", "py1", "sw0", "x332e", "px0", "y32e", "py2", "sw1",
    "x322e", "px2", "sw2", "m0", "m1", "m2",
)


def rotation_tables():
    f32 = np.float32
    freqs = (f32(ROPE_BASE) ** (-np.arange(0, HEAD_DIM, 2, dtype=f32) / f32(HEAD_DIM))).astype(f32)
    lanes = np.tile(freqs.astype(np.float64), 4)
    inner = np.arange(ROWS)[:, None] * lanes[None]
    outer = (np.arange(SEQLEN // ROWS) * ROWS)[:, None] * lanes[None]
    inner = np.stack([np.cos(inner), np.sin(inner)]).astype(f32)
    outer = np.stack([np.cos(outer), np.sin(outer)], 1).astype(f32)
    return inner, outer


def kernel(
    lam_hbm, q_hbm, k_hbm, v_hbm, gain_hbm, inner_hbm, outer_hbm, w_hbm,
    out_ref,
    lam_ref, gain_ref, inner_ref, outer_ref, q_in, k_in, v_in,
    kvst, kv, qst, qin, q2, sbuf, acc, wbuf, hst, acts, pacc, oown, opart, oin,
    in_sem, sent, kvz_r, kvy_r, q_r, ring_r, fin_r, oz_r, af_r, oo_r,
):
    f32, bf16 = jnp.float32, jnp.bfloat16
    sp, dp = lax.axis_index("sp"), lax.axis_index("dp")
    me = {"z": sp // 4, "y": lax.rem(sp, 4), "x": dp // 2}
    core = lax.rem(dp, 2)

    def at(pos):
        return (pos["z"] * 4 + pos["y"], pos["x"] * 2 + core)

    def shift(dim, off):
        return {**me, dim: lax.rem(me[dim] + off + 4, 4)}

    partner = (sp, me["x"] * 2 + 1 - core)
    total_sent = [0, 0]

    def size(ref):
        return int(np.prod(ref.shape)) * ref.dtype.itemsize

    def amount(nbytes):
        rows = nbytes // 4096
        n = 1 if rows <= KT else (2 if rows % 16 == 0 and rows <= 2 * KT else 4)
        assert rows * 4096 == nbytes and rows % n == 0
        return sbuf.at[pl.ds(0, n), pl.ds(0, rows // n), :]

    def send(src, dst, r_sem, dev, kind=0):
        total_sent[kind] += size(src)
        pltpu.make_async_remote_copy(
            src_ref=src, dst_ref=dst, send_sem=sent.at[kind], recv_sem=r_sem, device_id=dev, device_id_type=MESH
        ).start()

    def arrived(nbytes, r_sem, name="wait"):
        view = amount(nbytes)
        with jax.named_scope(name):
            pltpu.make_async_remote_copy(
                src_ref=view, dst_ref=view, send_sem=sent.at[0], recv_sem=r_sem, device_id=partner, device_id_type=MESH
            ).wait_recv()

    barrier = pltpu.get_barrier_semaphore()
    peers = [at(shift("z", o)) for o in (1, 2, 3)] + [at(shift("y", o)) for o in ((1, 2, 3) if DIRECT else (1, 3))]
    peers += [at(shift("x", o)) for o in (1, 3)] + [partner]
    for dev in peers:
        pl.semaphore_signal(barrier, inc=1, device_id=dev, device_id_type=MESH)

    copies = [
        pltpu.make_async_copy(src, dst, in_sem.at[n])
        for n, (src, dst) in enumerate((
            (k_hbm, k_in),
            (inner_hbm, inner_ref),
            (outer_hbm.at[sp], outer_ref),
            (v_hbm, v_in),
            (w_hbm, wbuf.at[me["z"], me["y"], me["x"]]),
            (q_hbm, q_in),
            (gain_hbm, gain_ref),
            (lam_hbm, lam_ref),
        ))
    ]
    for c in copies:
        c.start()
    c_k, c_in, c_out, c_v, c_w, c_q, c_gain, c_lam = copies
    with jax.named_scope("barrier"):
        pl.semaphore_wait(barrier, len(peers))

    def rotate(part):
        turned = jnp.dot(part, kept["swap"], preferred_element_type=f32)
        return (part.astype(f32) * kept["cosine"] + turned * kept["sine"]).astype(bf16)

    kept = {}

    def rotate_keys():
        with jax.named_scope("rotk"):
            row = lax.broadcasted_iota(jnp.int32, (128, 128), 0)
            col = lax.broadcasted_iota(jnp.int32, (128, 128), 1)
            low = lax.rem(col, 64) < 32
            kept["swap"] = jnp.where(
                low & (row == col + 32), -1.0, jnp.where(jnp.logical_not(low) & (row == col - 32), 1.0, 0.0)
            ).astype(bf16)
            c_v.wait()
            for g in range(KV_HEADS):
                kvst[g, 1] = v_in[:, g * 128:(g + 1) * 128].astype(f32).T.astype(bf16)
            c_in.wait()
            c_out.wait()
            ci, si = inner_ref[0], inner_ref[1]
            co, so = outer_ref[0:1, :], outer_ref[1:2, :]
            kept["cosine"] = co * ci - so * si
            kept["sine"] = so * ci + co * si
            c_k.wait()
            for g in range(KV_HEADS):
                kvst[g, 0] = rotate(k_in[:, g * 128:(g + 1) * 128])
            kv[sp, 0] = kvst[me["z"], 0]
            kv[sp, 1] = kvst[me["z"], 1]
            c_w.wait()

    steps = (0, 3, 1, 2)
    block_bytes = size(kv.at[0])

    def kv_block(rel, off):
        return lax.rem(me["z"] + rel, 4) * 4 + lax.rem(me["y"] + off + 4, 4)

    def kvz_start(o):
        pos = shift("z", o)
        send(kvst.at[pos["z"]], kv.at[sp], kvz_r.at[o - 1], at(pos))

    def kvz_wait(rel):
        arrived(block_bytes, kvz_r.at[3 - rel], f"kvz_{rel}")

    def kvy_start(rel):
        view = kvst.at[me["z"]] if rel == 0 else kv.at[kv_block(rel, 0)]
        for off in (1, -1):
            send(view, kv.at[kv_block(rel, 0)], kvy_r.at[4 if rel in DIRECT else rel], at(shift("y", off)))
        if rel in DIRECT:
            send(view, kv.at[kv_block(rel, 0)], kvy_r.at[4], at(shift("y", 2)))

    def kvy_forward(rel):
        arrived(2 * block_bytes, kvy_r.at[rel], f"kvy_{rel}")
        for n, off in enumerate((-1, 1)):
            half = kv.at[kv_block(rel, off), n]
            send(half, half, kvy_r.at[4], at(shift("y", -off)))

    made = []

    class Ring:
        def __init__(self, colour, dim, fin, **fixed):
            self.dim, self.fixed = dim, fixed
            self.k0, self.kn = COLOURS[colour]
            self.full, self.fin = ring_r.at[len(made)], fin_r.at[fin]
            self.bytes = size(self.view(0))
            self.name = f"{len(made)}{dim}"
            made.append(self)

        def view(self, off, half=None):
            sel, rows = {}, slice(None)
            for d in "zyx":
                rel = off if d == self.dim else self.fixed[d]
                sel[d] = slice(None) if rel is None else lax.rem(me[d] + rel + 4, 4)
            if half is not None:
                free = [d for d in "zyx" if d != self.dim and self.fixed[d] is None]
                if free:
                    sel[free[0]] = pl.ds(2 * half, 2)
                else:
                    rows = pl.ds(16 * half, 16)
            return wbuf.at[sel["z"], sel["y"], sel["x"], rows, pl.ds(self.k0, self.kn)]

        def start(self):
            view = src = self.view(0)
            if all(r == 0 for r in self.fixed.values()):
                src = w_hbm.at[:, pl.ds(self.k0, self.kn)]
            for off in (1, -1):
                send(src, view, self.full, at(shift(self.dim, off)), 1)

        def forward(self):
            arrived(2 * self.bytes, self.full, "fwd" + self.name)
            for n, off in enumerate((-1, 1)):
                half = self.view(off, n)
                send(half, half, self.fin, at(shift(self.dim, -off)), 1)

        def finish(self):
            arrived(self.bytes, self.fin, "fin" + self.name)

    x1 = Ring(0, "z", 0, y=0, x=0)
    x2 = {a: Ring(0, "y", 1 + a, z=a, x=0) for a in steps}
    x3 = {(a, b): Ring(0, "x", 21 + a if b == 2 else 5 + b, z=a, y=b) for b in steps for a in steps}
    y1 = Ring(1, "x", 9, z=0, y=0)
    y2 = Ring(1, "z", 10, x=None, y=0)
    y3 = {a: Ring(1, "y", 11 + a, x=None, z=a) for a in steps}
    z1 = Ring(2, "x", 15, z=0, y=0)
    z2 = Ring(2, "y", 16, x=None, z=0)
    z3 = {b: Ring(2, "z", 17 + b, x=None, y=b) for b in steps}

    def x3_finish(b):
        arrived(4 * x3[0, b].bytes, x3[0, b].fin, f"finx{b}")

    tasks = {"kvzs": lambda: [kvz_start(o) for o in (1, 3, 2)]}
    for a in steps:
        tasks[f"kvz{a}w"] = functools.partial(kvz_wait, a)
        tasks[f"kvy{a}s"] = functools.partial(kvy_start, a)
        if a not in DIRECT:
            tasks[f"kvy{a}f"] = functools.partial(kvy_forward, a)
    tasks["kvall"] = lambda: arrived((4 + 2 * len(DIRECT)) * block_bytes, kvy_r.at[4], "kvyf")
    rings = {"x1": x1, "y1": y1, "z1": z1, "y2": y2, "z2": z2}
    for a in steps:
        rings.update({f"x2{a}": x2[a], f"y3{a}": y3[a], f"z3{a}": z3[a]})
        rings.update({f"x3{a}{b}": x3[a, b] for b in steps})
    for name, ring in rings.items():
        tasks.update({name + "s": ring.start, name + "f": ring.forward, name + "e": ring.finish})

    def rotate_queries():
        with jax.named_scope("rotq"):
            c_q.wait()
            for g in range(KV_HEADS):
                for h in range(GROUP):
                    a = (g * GROUP + h) * 128
                    qst[g, :, h * 128:(h + 1) * 128] = rotate(q_in[:, a:a + 128])
            qin[me["z"]] = qst[me["z"]]
            pacc[...] = jnp.zeros_like(pacc)

    def send_queries():
        for o in (1, 3, 2):
            pos = shift("z", o)
            send(qst.at[pos["z"]], qin.at[me["z"]], q_r.at[o - 1], at(pos))

    tasks.update({"rotk": rotate_keys, "rotq": rotate_queries, "qs": send_queries})

    scale = float(HEAD_DIM ** -0.5 * np.log2(np.e))
    c_lam.wait()
    lam = jnp.concatenate(
        [jnp.full((1, 128), lam_ref[me["z"] * GROUP + h], f32) for h in range(GROUP)], 1
    )
    lane = lax.broadcasted_iota(jnp.int32, (128, 128), 1)
    half_rows = GROUP * ROWS

    def fold(x, op):
        return op(x.reshape(KT // 8, 8, x.shape[1]), 0)

    def attend_scores(i):
        zq = lax.rem(me["z"] + 1 + i, 4)
        if i < 3:
            o = 3 - i
            arrived(size(qin.at[0]), q_r.at[o - 1], f"q_{i}")
        for m in range(2):
            keep = (lane < 64) if m == 0 else (lane >= 64)
            for h in range(GROUP):
                part = qin[zq, :, h * 128:(h + 1) * 128]
                q2[(m * GROUP + h) * 128:(m * GROUP + h + 1) * 128, :] = jnp.where(
                    keep, part, jnp.zeros_like(part)
                )
        block = zq * 4 + me["y"]
        last = zq

        def scores(t):
            keys = jnp.concatenate([kv[4 * t + b, 0] for b in range(4)], 0)
            return lax.dot_general(keys, q2[...], (((1,), (1,)), ((), ())), preferred_element_type=f32)

        def pass1(t, top):
            s = scores(t)
            sbuf[t] = s
            return jnp.maximum(top, fold(s, jnp.max))

        top = lax.fori_loop(0, last, pass1, jnp.full((8, 2 * half_rows), -1e30, f32))
        s = scores(last)
        key_at = lax.broadcasted_iota(jnp.int32, (KT, 2 * half_rows), 0) + last * KT
        query_at = lax.rem(lax.broadcasted_iota(jnp.int32, (KT, 2 * half_rows), 1), 128) + block * 128
        s = jnp.where(key_at <= query_at, s, -1e30)
        sbuf[last] = s
        top = jnp.maximum(top, fold(s, jnp.max))
        top = jnp.max(top, 0, keepdims=True)
        kept["top"] = top

    def attend_exp(i):
        last = lax.rem(me["z"] + 1 + i, 4)
        top = kept["top"]

        def pass2(t, total):
            p = jnp.exp2((sbuf[t] - top) * scale)
            sbuf[t] = p
            return total + fold(p, jnp.sum)

        total = lax.fori_loop(0, last + 1, pass2, jnp.zeros((8, 2 * half_rows), f32))
        kept["total"] = jnp.sum(total, 0, keepdims=True)

    def attend_values(i):
        zq = last = lax.rem(me["z"] + 1 + i, 4)
        total = kept["total"]
        a0 = 1.0 / total[:, :half_rows]
        a1 = lam / total[:, half_rows:]
        acc[...] = jnp.zeros_like(acc)

        def pass3(t, carry):
            w = (sbuf[t, :, :half_rows] * a0 - sbuf[t, :, half_rows:] * a1).astype(bf16)
            vals = jnp.concatenate([kv[4 * t + b, 1] for b in range(4)], 1)
            acc[...] += jnp.dot(vals, w, preferred_element_type=f32)
            return carry

        lax.fori_loop(0, last + 1, pass3, 0)
        hv = acc[...]
        inv = lax.rsqrt(jnp.mean(hv * hv, 0, keepdims=True) + NORM_EPS)
        hv = hv * inv
        for h in range(GROUP):
            piece = hv[:, h * 128:(h + 1) * 128].T
            hst[zq, :, h * 128:(h + 1) * 128] = (piece * gain_ref[...] * OUTPUT_SCALE).astype(bf16)
        ship(i, zq)

    def ship(i, zq):
        if i < 3:
            o = i + 1
            send(hst.at[zq], acts.at[0, me["z"]], oz_r.at[o - 1], at(shift("z", o)))
        else:
            acts[0, me["z"]] = hst[me["z"]]
            send(hst.at[me["z"]], acts.at[1, me["z"]], af_r.at[0], partner)

    def acts_in(o):
        g = lax.rem(me["z"] + 4 - o, 4)
        arrived(size(acts.at[0, 0]), oz_r.at[o - 1], f"o_{o}")
        send(acts.at[0, g], acts.at[1, g], af_r.at[0], partner)

    def multiply(heads, weights):
        total = None
        for n, g in enumerate(heads):
            part = lax.dot_general(
                acts[:, g].reshape(2 * ROWS, 512), weights[:, n * 512:(n + 1) * 512],
                (((1,), (1,)), ((), ())), preferred_element_type=f32,
            )
            total = part if total is None else total + part
        return total

    def project_xz(b):
        with jax.named_scope(f"proj_xz{b}"):
            yb = lax.rem(me["y"] + b, 4)
            cat = lambda lo, hi: jnp.concatenate(
                [wbuf[z, yb, :, :, lo:hi].reshape(128, hi - lo) for z in range(4)], 0
            )
            part = multiply((0, 1), cat(0, 1024)) + multiply((3,), cat(1536, 2048))
            for z in range(4):
                pacc[z, yb] += part[:, z * 128:(z + 1) * 128]

    def project_x(places):
        with jax.named_scope(f"proj_x{places[0]}"):
            spots = [tile_of(a, 2) for a in places]
            cat = jnp.concatenate([wbuf[z, y, :, :, 0:1024].reshape(128, 1024) for z, y in spots], 0)
            part = multiply((0, 1), cat)
            for n, (z, y) in enumerate(spots):
                pacc[z, y] += part[:, n * 128:(n + 1) * 128]

    def project_z(b):
        with jax.named_scope(f"proj_z{b}"):
            yb = lax.rem(me["y"] + b, 4)
            cat = jnp.concatenate([wbuf[z, yb, :, :, 1536:2048].reshape(128, 512) for z in range(4)], 0)
            part = multiply((3,), cat)
            for z in range(4):
                pacc[z, yb] += part[:, z * 128:(z + 1) * 128]

    def project_y(a):
        with jax.named_scope(f"proj_y{a}"):
            za = lax.rem(me["z"] + a, 4)
            part = multiply((2,), wbuf[za, :, :, :, 1024:1536].reshape(512, 512))
            for y in range(4):
                pacc[za, y] += part[:, y * 128:(y + 1) * 128]

    early = [(a, b) for a in (0, 3, 1) for b in (0, 3, 1)]
    late = [(2, b) for b in (0, 3, 1)] + [(a, 2) for a in (0, 3, 1)]

    def tile_of(a, b):
        return lax.rem(me["z"] + a, 4), lax.rem(me["y"] + b, 4)

    def swap_tiles(tiles, n):
        for a, b in tiles:
            z, y = tile_of(a, b)
            opart[z, y] = pacc[z, y, ROWS:].astype(bf16)
        for a, b in tiles:
            z, y = tile_of(a, b)
            send(opart.at[z, y], oin.at[z, y], oo_r.at[n], partner)
            oown[z, y] = pacc[z, y, :ROWS].astype(bf16)

    erow = lax.broadcasted_iota(jnp.int32, (256, 256), 0)
    ecol = lax.broadcasted_iota(jnp.int32, (256, 256), 1)
    mine = jnp.where(erow < 128, core, 1 - core)
    er = lax.rem(erow, 128)
    spread = jnp.where(ecol == (er // 32) * 64 + mine * 32 + lax.rem(er, 32), 1.0, 0.0).astype(bf16)

    def merge(tiles, n):
        arrived(len(tiles) * size(oin.at[0, 0]), oo_r.at[n], f"swap_{n}")
        with jax.named_scope(f"merge_{n}"):
            for a, b in tiles:
                z, y = tile_of(a, b)
                both = jnp.concatenate([oown[z, y], oin[z, y]], 1)
                cols = pl.ds(pl.multiple_of((z * 4 + y) * 256, 256), 256)
                out_ref[:, cols] = jnp.dot(both, spread, preferred_element_type=f32).astype(bf16)

    def scoped(name, fn, *args):
        with jax.named_scope(name):
            fn(*args)

    def project_xz_task(b):
        x3_finish(b)
        project_xz(b)

    for i in range(4):
        for n, fn in enumerate((attend_scores, attend_exp, attend_values)):
            tasks[f"at{i}{n}"] = functools.partial(scoped, f"at{i}{n}", fn, i)
    for o in (1, 2, 3):
        tasks[f"o{o}w"] = functools.partial(acts_in, o)
    tasks["acts"] = lambda: arrived(4 * size(acts.at[0, 0]), af_r.at[0], "acts")
    for b in steps:
        tasks[f"pxz{b}"] = functools.partial(project_xz_task, b)
        tasks[f"py{b}"] = functools.partial(project_y, b)
    del tasks["pxz2"]
    tasks["px0"] = functools.partial(project_x, (0, 3, 1))
    tasks["px2"] = functools.partial(project_x, (2,))
    tasks["pz2"] = functools.partial(project_z, 2)
    for n, tiles in enumerate((early, late, [(2, 2)])):
        tasks[f"sw{n}"] = functools.partial(swap_tiles, tiles, n)
        tasks[f"m{n}"] = functools.partial(merge, tiles, n)
    c_gain.wait()
    left = [n for n in tasks if not (n.startswith("x3") and n.endswith("e") and n[3] != "2")]
    left.remove("kvz0w")
    assert sorted(left) == sorted(ORDER)
    for name in ORDER:
        tasks[name]()
    with jax.named_scope("drain"):
        for kind in (0, 1):
            view = amount(total_sent[kind])
            pltpu.make_async_remote_copy(
                src_ref=view, dst_ref=view, send_sem=sent.at[kind], recv_sem=oo_r.at[0],
                device_id=partner, device_id_type=MESH,
            ).wait_send()


def shards(queries, keys, values, lambdas, value_gain, out_weight):
    inner, outer = rotation_tables()
    vmem = pl.BlockSpec(memory_space=pltpu.VMEM)
    hbm = pl.BlockSpec(memory_space=pltpu.HBM)
    bf16, f32 = jnp.bfloat16, jnp.float32
    dma = lambda n: pltpu.SemaphoreType.DMA((n,))
    out = pl.pallas_call(
        kernel,
        out_shape=jax.ShapeDtypeStruct((ROWS, D), bf16),
        in_specs=[hbm] * 8,
        out_specs=vmem,
        scratch_shapes=[
            pltpu.SMEM((HEADS,), f32),
            pltpu.VMEM((1, 128), f32),
            pltpu.VMEM((2, ROWS, 128), f32),
            pltpu.VMEM((2, 128), f32),
            pltpu.VMEM((ROWS, 2048), bf16),
            pltpu.VMEM((ROWS, 512), bf16),
            pltpu.VMEM((ROWS, 512), bf16),
            pltpu.VMEM((4, 2, 128, 128), bf16),
            pltpu.VMEM((16, 2, 128, 128), bf16),
            pltpu.VMEM((4, 128, 512), bf16),
            pltpu.VMEM((4, 128, 512), bf16),
            pltpu.VMEM((1024, 128), bf16),
            pltpu.VMEM((SEQLEN // KT, KT, 1024), f32),
            pltpu.VMEM((128, 512), f32),
            pltpu.VMEM((4, 4, 4, 32, 2048), bf16),
            pltpu.VMEM((4, 128, 512), bf16),
            pltpu.VMEM((2, 4, 128, 512), bf16),
            pltpu.VMEM((4, 4, 256, 128), f32),
            pltpu.VMEM((4, 4, 128, 128), bf16),
            pltpu.VMEM((4, 4, 128, 128), bf16),
            pltpu.VMEM((4, 4, 128, 128), bf16),
            dma(8), dma(2), dma(3), dma(5), dma(3), dma(33), dma(25), dma(3), dma(1), dma(3),
        ],
        compiler_params=pltpu.CompilerParams(
            collective_id=0, has_side_effects=True, vmem_limit_bytes=50_000_000
        ),
        name="layer",
    )(*(
        pltpu.with_memory_space_constraint(a, pltpu.HBM)
        for a in (
            lambdas, queries[0], keys[0], values[0], value_gain.reshape(1, 128),
            jnp.asarray(inner), jnp.asarray(outer), out_weight.T,
        )
    ))
    return out[None]


def solution(mesh):
    return jax.shard_map(
        shards,
        mesh=mesh,
        in_specs=(
            P("dp", "sp", None),
            P("dp", "sp", None),
            P("dp", "sp", None),
            P(),
            P(),
            P(None, ("sp", "dp")),
        ),
        out_specs=P("dp", "sp", None),
        check_vma=False,
    )
```

```python
import functools

import jax
import jax.numpy as jnp
import numpy as np
from jax import lax
from jax.experimental import pallas as pl
from jax.experimental.pallas import tpu as pltpu
from jax.sharding import PartitionSpec as P

HEADS = 16
KV_HEADS = 4
HEAD_DIM = 64
VALUE_DIM = 128
D = 4096
SEQLEN = 2048
ROWS = 128
GROUP = HEADS // KV_HEADS
KT = 512
ROPE_BASE = 500000.0
OUTPUT_SCALE = 0.8
NORM_EPS = 1e-05
MESH = pl.DeviceIdType.MESH

COLOURS = ((0, 1024), (1024, 512), (1536, 512))

DIRECT = ()
ORDER = (
    "x20s", "x1s", "z1s", "y1s", "x300s", "rotk", "kvzs", "kvy0s", "rotq", "kvy0f", "kvz3w", "kvy3s", "qs",
    "kvz1w", "z1f", "kvy1s", "x20f", "x301s", "x1f", "x310s", "x303s", "y1f", "x330s", "kvz2w", "kvy2s",
    "x300f", "z1e", "z30s", "kvy3f", "x301f", "kvy1f", "x23s", "x310f", "x20e", "x302s", "x303f", "y1e",
    "y2s", "kvy2f", "z2s", "x21s", "x1e", "x22s", "x320s", "x330f", "x23f", "x331s", "x333s", "kvall", "at00",
    "z30f", "x302f", "at01", "at02", "y2f", "y33s", "z2f", "z33s", "at10", "x21f", "x313s", "x311s", "at11",
    "at12", "x331f", "x22f", "x323s", "y31s", "x321s", "z31s", "z30e", "at20", "x23e", "x332s", "x333f",
    "at21", "at22", "x313f", "y30s", "o1w", "at30", "y2e", "y32s", "at31", "at32", "x22e", "x322s", "y33f",
    "z2e", "z32s", "x21e", "x311f", "x302e", "x320f", "x312s", "x323f", "z33f", "x321f", "y31f", "x332f",
    "o2w", "y30f", "x322f", "z31f", "o3w", "acts", "pxz0", "y32f", "x312f", "z32f", "y33e", "py3", "z33e",
    "pxz3", "x332e", "y31e", "py1", "x322e", "px2", "z31e", "pxz1", "y30e", "py0", "sw0", "x312e", "px0",
    "z32e", "pz2", "sw1", "y32e", "py2", "sw2", "m0", "m1", "m2",
)


def rotation_tables():
    f32 = np.float32
    freqs = (f32(ROPE_BASE) ** (-np.arange(0, HEAD_DIM, 2, dtype=f32) / f32(HEAD_DIM))).astype(f32)
    lanes = np.tile(freqs.astype(np.float64), 4)
    inner = np.arange(ROWS)[:, None] * lanes[None]
    outer = (np.arange(SEQLEN // ROWS) * ROWS)[:, None] * lanes[None]
    inner = np.stack([np.cos(inner), np.sin(inner)]).astype(f32)
    outer = np.stack([np.cos(outer), np.sin(outer)], 1).astype(f32)
    return inner, outer


def kernel(
    lam_hbm, q_hbm, k_hbm, v_hbm, gain_hbm, inner_hbm, outer_hbm, w_hbm,
    out_ref,
    lam_ref, gain_ref, inner_ref, outer_ref, q_in, k_in, v_in,
    kvst, kv, qst, qin, q2, sbuf, acc, wbuf, hst, acts, pacc, oown, opart, oin,
    in_sem, sent, kvz_r, kvy_r, q_r, ring_r, fin_r, oz_r, af_r, oo_r,
):
    f32, bf16 = jnp.float32, jnp.bfloat16
    sp, dp = lax.axis_index("sp"), lax.axis_index("dp")
    me = {"z": sp // 4, "y": lax.rem(sp, 4), "x": dp // 2}
    core = lax.rem(dp, 2)

    def at(pos):
        return (pos["z"] * 4 + pos["y"], pos["x"] * 2 + core)

    def shift(dim, off):
        return {**me, dim: lax.rem(me[dim] + off + 4, 4)}

    partner = (sp, me["x"] * 2 + 1 - core)
    total_sent = [0, 0]

    def size(ref):
        return int(np.prod(ref.shape)) * ref.dtype.itemsize

    def amount(nbytes):
        rows = nbytes // 4096
        n = 1 if rows <= KT else (2 if rows % 16 == 0 and rows <= 2 * KT else 4)
        assert rows * 4096 == nbytes and rows % n == 0
        return sbuf.at[pl.ds(0, n), pl.ds(0, rows // n), :]

    def send(src, dst, r_sem, dev, kind=0):
        total_sent[kind] += size(src)
        pltpu.make_async_remote_copy(
            src_ref=src, dst_ref=dst, send_sem=sent.at[kind], recv_sem=r_sem, device_id=dev, device_id_type=MESH
        ).start()

    def arrived(nbytes, r_sem, name="wait"):
        view = amount(nbytes)
        with jax.named_scope(name):
            pltpu.make_async_remote_copy(
                src_ref=view, dst_ref=view, send_sem=sent.at[0], recv_sem=r_sem, device_id=partner, device_id_type=MESH
            ).wait_recv()

    barrier = pltpu.get_barrier_semaphore()
    peers = [at(shift("z", o)) for o in (1, 2, 3)] + [at(shift("y", o)) for o in ((1, 2, 3) if DIRECT else (1, 3))]
    peers += [at(shift("x", o)) for o in (1, 3)] + [partner]
    for dev in peers:
        pl.semaphore_signal(barrier, inc=1, device_id=dev, device_id_type=MESH)

    copies = [
        pltpu.make_async_copy(src, dst, in_sem.at[n])
        for n, (src, dst) in enumerate((
            (k_hbm, k_in),
            (inner_hbm, inner_ref),
            (outer_hbm.at[sp], outer_ref),
            (v_hbm, v_in),
            (w_hbm, wbuf.at[me["z"], me["y"], me["x"]]),
            (q_hbm, q_in),
            (gain_hbm, gain_ref),
            (lam_hbm, lam_ref),
        ))
    ]
    for c in copies:
        c.start()
    c_k, c_in, c_out, c_v, c_w, c_q, c_gain, c_lam = copies
    with jax.named_scope("barrier"):
        pl.semaphore_wait(barrier, len(peers))

    def rotate(part):
        turned = jnp.dot(part, kept["swap"], preferred_element_type=f32)
        return (part.astype(f32) * kept["cosine"] + turned * kept["sine"]).astype(bf16)

    kept = {}

    def rotate_keys():
        with jax.named_scope("rotk"):
            row = lax.broadcasted_iota(jnp.int32, (128, 128), 0)
            col = lax.broadcasted_iota(jnp.int32, (128, 128), 1)
            low = lax.rem(col, 64) < 32
            kept["swap"] = jnp.where(
                low & (row == col + 32), -1.0, jnp.where(jnp.logical_not(low) & (row == col - 32), 1.0, 0.0)
            ).astype(bf16)
            c_v.wait()
            for g in range(KV_HEADS):
                kvst[g, 1] = v_in[:, g * 128:(g + 1) * 128].astype(f32).T.astype(bf16)
            c_in.wait()
            c_out.wait()
            ci, si = inner_ref[0], inner_ref[1]
            co, so = outer_ref[0:1, :], outer_ref[1:2, :]
            kept["cosine"] = co * ci - so * si
            kept["sine"] = so * ci + co * si
            c_k.wait()
            for g in range(KV_HEADS):
                kvst[g, 0] = rotate(k_in[:, g * 128:(g + 1) * 128])
            kv[sp, 0] = kvst[me["z"], 0]
            kv[sp, 1] = kvst[me["z"], 1]
            c_w.wait()

    steps = (0, 3, 1, 2)
    block_bytes = size(kv.at[0])

    def kv_block(rel, off):
        return lax.rem(me["z"] + rel, 4) * 4 + lax.rem(me["y"] + off + 4, 4)

    def kvz_start(o):
        pos = shift("z", o)
        send(kvst.at[pos["z"]], kv.at[sp], kvz_r.at[o - 1], at(pos))

    def kvz_wait(rel):
        arrived(block_bytes, kvz_r.at[3 - rel], f"kvz_{rel}")

    def kvy_start(rel):
        view = kvst.at[me["z"]] if rel == 0 else kv.at[kv_block(rel, 0)]
        for off in (1, -1):
            send(view, kv.at[kv_block(rel, 0)], kvy_r.at[4 if rel in DIRECT else rel], at(shift("y", off)))
        if rel in DIRECT:
            send(view, kv.at[kv_block(rel, 0)], kvy_r.at[4], at(shift("y", 2)))

    def kvy_forward(rel):
        arrived(2 * block_bytes, kvy_r.at[rel], f"kvy_{rel}")
        for n, off in enumerate((-1, 1)):
            half = kv.at[kv_block(rel, off), n]
            send(half, half, kvy_r.at[4], at(shift("y", -off)))

    made = []

    class Ring:
        def __init__(self, colour, dim, fin, **fixed):
            self.dim, self.fixed = dim, fixed
            self.k0, self.kn = COLOURS[colour]
            self.full, self.fin = ring_r.at[len(made)], fin_r.at[fin]
            self.bytes = size(self.view(0))
            self.name = f"{len(made)}{dim}"
            made.append(self)

        def view(self, off, half=None):
            sel, rows = {}, slice(None)
            for d in "zyx":
                rel = off if d == self.dim else self.fixed[d]
                sel[d] = slice(None) if rel is None else lax.rem(me[d] + rel + 4, 4)
            if half is not None:
                free = [d for d in "zyx" if d != self.dim and self.fixed[d] is None]
                if free:
                    sel[free[0]] = pl.ds(2 * half, 2)
                else:
                    rows = pl.ds(16 * half, 16)
            return wbuf.at[sel["z"], sel["y"], sel["x"], rows, pl.ds(self.k0, self.kn)]

        def start(self):
            view = src = self.view(0)
            if all(r == 0 for r in self.fixed.values()):
                src = w_hbm.at[:, pl.ds(self.k0, self.kn)]
            for off in (1, -1):
                send(src, view, self.full, at(shift(self.dim, off)), 1)

        def forward(self):
            arrived(2 * self.bytes, self.full, "fwd" + self.name)
            for n, off in enumerate((-1, 1)):
                half = self.view(off, n)
                send(half, half, self.fin, at(shift(self.dim, -off)), 1)

        def finish(self):
            arrived(self.bytes, self.fin, "fin" + self.name)

    x1 = Ring(0, "z", 0, y=0, x=0)
    x2 = {a: Ring(0, "y", 1 + a, z=a, x=0) for a in steps}
    x3 = {(a, b): Ring(0, "x", 21 + a if b == 2 else 5 + b, z=a, y=b) for b in steps for a in steps}
    y1 = Ring(1, "x", 9, z=0, y=0)
    y2 = Ring(1, "z", 10, x=None, y=0)
    y3 = {a: Ring(1, "y", 11 + a, x=None, z=a) for a in steps}
    z1 = Ring(2, "x", 15, z=0, y=0)
    z2 = Ring(2, "y", 16, x=None, z=0)
    z3 = {b: Ring(2, "z", 17 + b, x=None, y=b) for b in steps}

    def x3_finish(b):
        arrived(4 * x3[0, b].bytes, x3[0, b].fin, f"finx{b}")

    tasks = {"kvzs": lambda: [kvz_start(o) for o in (1, 3, 2)]}
    for a in steps:
        tasks[f"kvz{a}w"] = functools.partial(kvz_wait, a)
        tasks[f"kvy{a}s"] = functools.partial(kvy_start, a)
        if a not in DIRECT:
            tasks[f"kvy{a}f"] = functools.partial(kvy_forward, a)
    tasks["kvall"] = lambda: arrived((4 + 2 * len(DIRECT)) * block_bytes, kvy_r.at[4], "kvyf")
    rings = {"x1": x1, "y1": y1, "z1": z1, "y2": y2, "z2": z2}
    for a in steps:
        rings.update({f"x2{a}": x2[a], f"y3{a}": y3[a], f"z3{a}": z3[a]})
        rings.update({f"x3{a}{b}": x3[a, b] for b in steps})
    for name, ring in rings.items():
        tasks.update({name + "s": ring.start, name + "f": ring.forward, name + "e": ring.finish})

    def rotate_queries():
        with jax.named_scope("rotq"):
            c_q.wait()
            for g in range(KV_HEADS):
                for h in range(GROUP):
                    a = (g * GROUP + h) * 128
                    qst[g, :, h * 128:(h + 1) * 128] = rotate(q_in[:, a:a + 128])
            qin[me["z"]] = qst[me["z"]]
            pacc[...] = jnp.zeros_like(pacc)

    def send_queries():
        for o in (1, 3, 2):
            pos = shift("z", o)
            send(qst.at[pos["z"]], qin.at[me["z"]], q_r.at[o - 1], at(pos))

    tasks.update({"rotk": rotate_keys, "rotq": rotate_queries, "qs": send_queries})

    scale = float(HEAD_DIM ** -0.5 * np.log2(np.e))
    half_rows = GROUP * ROWS

    def fold(x, op):
        return op(x.reshape(KT // 8, 8, x.shape[1]), 0)

    def attend_scores(i):
        zq = lax.rem(me["z"] + 1 + i, 4)
        if i < 3:
            o = 3 - i
            arrived(size(qin.at[0]), q_r.at[o - 1], f"q_{i}")
        lane = lax.broadcasted_iota(jnp.int32, (128, 128), 1)
        for m in range(2):
            keep = (lane < 64) if m == 0 else (lane >= 64)
            for h in range(GROUP):
                part = qin[zq, :, h * 128:(h + 1) * 128]
                q2[(m * GROUP + h) * 128:(m * GROUP + h + 1) * 128, :] = jnp.where(
                    keep, part, jnp.zeros_like(part)
                )
        block = zq * 4 + me["y"]
        last = zq

        def scores(t):
            keys = jnp.concatenate([kv[4 * t + b, 0] for b in range(4)], 0)
            return lax.dot_general(keys, q2[...], (((1,), (1,)), ((), ())), preferred_element_type=f32)

        def pass1(t, top):
            s = scores(t)
            sbuf[t] = s
            return jnp.maximum(top, fold(s, jnp.max))

        top = lax.fori_loop(0, last, pass1, jnp.full((8, 2 * half_rows), -1e30, f32))
        s = scores(last)
        key_at = lax.broadcasted_iota(jnp.int32, (KT, 2 * half_rows), 0) + last * KT
        query_at = lax.rem(lax.broadcasted_iota(jnp.int32, (KT, 2 * half_rows), 1), 128) + block * 128
        s = jnp.where(key_at <= query_at, s, -1e30)
        sbuf[last] = s
        top = jnp.maximum(top, fold(s, jnp.max))
        top = jnp.max(top, 0, keepdims=True)
        kept["top"] = top

    def attend_exp(i):
        last = lax.rem(me["z"] + 1 + i, 4)
        top = kept["top"]

        def pass2(t, total):
            p = jnp.exp2((sbuf[t] - top) * scale)
            sbuf[t] = p
            return total + fold(p, jnp.sum)

        total = lax.fori_loop(0, last + 1, pass2, jnp.zeros((8, 2 * half_rows), f32))
        kept["total"] = jnp.sum(total, 0, keepdims=True)

    def attend_values(i):
        zq = last = lax.rem(me["z"] + 1 + i, 4)
        total = kept["total"]
        if i == 0:
            c_lam.wait()
            c_gain.wait()
        lam = jnp.concatenate(
            [jnp.full((1, 128), lam_ref[me["z"] * GROUP + h], f32) for h in range(GROUP)], 1
        )
        a0 = 1.0 / total[:, :half_rows]
        a1 = lam / total[:, half_rows:]
        acc[...] = jnp.zeros_like(acc)

        def pass3(t, carry):
            w = (sbuf[t, :, :half_rows] * a0 - sbuf[t, :, half_rows:] * a1).astype(bf16)
            vals = jnp.concatenate([kv[4 * t + b, 1] for b in range(4)], 1)
            acc[...] += jnp.dot(vals, w, preferred_element_type=f32)
            return carry

        lax.fori_loop(0, last + 1, pass3, 0)
        hv = acc[...]
        inv = lax.rsqrt(jnp.mean(hv * hv, 0, keepdims=True) + NORM_EPS)
        hv = hv * inv
        for h in range(GROUP):
            piece = hv[:, h * 128:(h + 1) * 128].T
            hst[zq, :, h * 128:(h + 1) * 128] = (piece * gain_ref[...] * OUTPUT_SCALE).astype(bf16)
        ship(i, zq)

    def ship(i, zq):
        if i < 3:
            o = i + 1
            send(hst.at[zq], acts.at[0, me["z"]], oz_r.at[o - 1], at(shift("z", o)))
        else:
            acts[0, me["z"]] = hst[me["z"]]
            send(hst.at[me["z"]], acts.at[1, me["z"]], af_r.at[0], partner)

    def acts_in(o):
        g = lax.rem(me["z"] + 4 - o, 4)
        arrived(size(acts.at[0, 0]), oz_r.at[o - 1], f"o_{o}")
        send(acts.at[0, g], acts.at[1, g], af_r.at[0], partner)

    def multiply(heads, weights):
        total = None
        for n, g in enumerate(heads):
            part = lax.dot_general(
                acts[:, g].reshape(2 * ROWS, 512), weights[:, n * 512:(n + 1) * 512],
                (((1,), (1,)), ((), ())), preferred_element_type=f32,
            )
            total = part if total is None else total + part
        return total

    def project_xz(b):
        with jax.named_scope(f"proj_xz{b}"):
            yb = lax.rem(me["y"] + b, 4)
            cat = lambda lo, hi: jnp.concatenate(
                [wbuf[z, yb, :, :, lo:hi].reshape(128, hi - lo) for z in range(4)], 0
            )
            part = multiply((0, 1), cat(0, 1024)) + multiply((3,), cat(1536, 2048))
            for z in range(4):
                pacc[z, yb] += part[:, z * 128:(z + 1) * 128]

    def project_x(places):
        with jax.named_scope(f"proj_x{places[0]}"):
            spots = [tile_of(a, 2) for a in places]
            cat = jnp.concatenate([wbuf[z, y, :, :, 0:1024].reshape(128, 1024) for z, y in spots], 0)
            part = multiply((0, 1), cat)
            for n, (z, y) in enumerate(spots):
                pacc[z, y] += part[:, n * 128:(n + 1) * 128]

    def project_z(b):
        with jax.named_scope(f"proj_z{b}"):
            yb = lax.rem(me["y"] + b, 4)
            cat = jnp.concatenate([wbuf[z, yb, :, :, 1536:2048].reshape(128, 512) for z in range(4)], 0)
            part = multiply((3,), cat)
            for z in range(4):
                pacc[z, yb] += part[:, z * 128:(z + 1) * 128]

    def project_y(a):
        with jax.named_scope(f"proj_y{a}"):
            za = lax.rem(me["z"] + a, 4)
            part = multiply((2,), wbuf[za, :, :, :, 1024:1536].reshape(512, 512))
            for y in range(4):
                pacc[za, y] += part[:, y * 128:(y + 1) * 128]

    early = [(a, b) for a in (0, 3, 1) for b in (0, 3, 1)]
    late = [(a, 2) for a in (0, 3, 1)]

    def tile_of(a, b):
        return lax.rem(me["z"] + a, 4), lax.rem(me["y"] + b, 4)

    def swap_tiles(tiles, n):
        for a, b in tiles:
            z, y = tile_of(a, b)
            opart[z, y] = pacc[z, y, ROWS:].astype(bf16)
        for a, b in tiles:
            z, y = tile_of(a, b)
            send(opart.at[z, y], oin.at[z, y], oo_r.at[n], partner)
            oown[z, y] = pacc[z, y, :ROWS].astype(bf16)

    def spread():
        erow = lax.broadcasted_iota(jnp.int32, (256, 256), 0)
        ecol = lax.broadcasted_iota(jnp.int32, (256, 256), 1)
        mine = jnp.where(erow < 128, core, 1 - core)
        er = lax.rem(erow, 128)
        return jnp.where(ecol == (er // 32) * 64 + mine * 32 + lax.rem(er, 32), 1.0, 0.0).astype(bf16)

    def merge(tiles, n):
        arrived(len(tiles) * size(oin.at[0, 0]), oo_r.at[n], f"swap_{n}")
        with jax.named_scope(f"merge_{n}"):
            if n == 0:
                kept["spread"] = spread()
            for a, b in tiles:
                z, y = tile_of(a, b)
                both = jnp.concatenate([oown[z, y], oin[z, y]], 1)
                cols = pl.ds(pl.multiple_of((z * 4 + y) * 256, 256), 256)
                out_ref[:, cols] = jnp.dot(both, kept["spread"], preferred_element_type=f32).astype(bf16)

    def scoped(name, fn, *args):
        with jax.named_scope(name):
            fn(*args)

    def project_xz_task(b):
        x3_finish(b)
        project_xz(b)

    for i in range(4):
        for n, fn in enumerate((attend_scores, attend_exp, attend_values)):
            tasks[f"at{i}{n}"] = functools.partial(scoped, f"at{i}{n}", fn, i)
    for o in (1, 2, 3):
        tasks[f"o{o}w"] = functools.partial(acts_in, o)
    tasks["acts"] = lambda: arrived(4 * size(acts.at[0, 0]), af_r.at[0], "acts")
    for b in steps:
        tasks[f"pxz{b}"] = functools.partial(project_xz_task, b)
        tasks[f"py{b}"] = functools.partial(project_y, b)
    del tasks["pxz2"]
    tasks["px0"] = functools.partial(project_x, (0, 3, 1))
    tasks["px2"] = functools.partial(project_x, (2,))
    tasks["pz2"] = functools.partial(project_z, 2)
    for n, tiles in enumerate((early, late, [(2, b) for b in steps])):
        tasks[f"sw{n}"] = functools.partial(swap_tiles, tiles, n)
        tasks[f"m{n}"] = functools.partial(merge, tiles, n)
    left = [n for n in tasks if not (n.startswith("x3") and n.endswith("e") and n[3] != "2")]
    left.remove("kvz0w")
    assert sorted(left) == sorted(ORDER)
    for name in ORDER:
        tasks[name]()
    with jax.named_scope("drain"):
        for kind in (0, 1):
            view = amount(total_sent[kind])
            pltpu.make_async_remote_copy(
                src_ref=view, dst_ref=view, send_sem=sent.at[kind], recv_sem=oo_r.at[0],
                device_id=partner, device_id_type=MESH,
            ).wait_send()


def shards(queries, keys, values, lambdas, value_gain, out_weight):
    inner, outer = rotation_tables()
    vmem = pl.BlockSpec(memory_space=pltpu.VMEM)
    hbm = pl.BlockSpec(memory_space=pltpu.HBM)
    bf16, f32 = jnp.bfloat16, jnp.float32
    dma = lambda n: pltpu.SemaphoreType.DMA((n,))
    out = pl.pallas_call(
        kernel,
        out_shape=jax.ShapeDtypeStruct((ROWS, D), bf16),
        in_specs=[hbm] * 8,
        out_specs=vmem,
        scratch_shapes=[
            pltpu.SMEM((HEADS,), f32),
            pltpu.VMEM((1, 128), f32),
            pltpu.VMEM((2, ROWS, 128), f32),
            pltpu.VMEM((2, 128), f32),
            pltpu.VMEM((ROWS, 2048), bf16),
            pltpu.VMEM((ROWS, 512), bf16),
            pltpu.VMEM((ROWS, 512), bf16),
            pltpu.VMEM((4, 2, 128, 128), bf16),
            pltpu.VMEM((16, 2, 128, 128), bf16),
            pltpu.VMEM((4, 128, 512), bf16),
            pltpu.VMEM((4, 128, 512), bf16),
            pltpu.VMEM((1024, 128), bf16),
            pltpu.VMEM((SEQLEN // KT, KT, 1024), f32),
            pltpu.VMEM((128, 512), f32),
            pltpu.VMEM((4, 4, 4, 32, 2048), bf16),
            pltpu.VMEM((4, 128, 512), bf16),
            pltpu.VMEM((2, 4, 128, 512), bf16),
            pltpu.VMEM((4, 4, 256, 128), f32),
            pltpu.VMEM((4, 4, 128, 128), bf16),
            pltpu.VMEM((4, 4, 128, 128), bf16),
            pltpu.VMEM((4, 4, 128, 128), bf16),
            dma(8), dma(2), dma(3), dma(5), dma(3), dma(33), dma(25), dma(3), dma(1), dma(3),
        ],
        compiler_params=pltpu.CompilerParams(
            collective_id=0, has_side_effects=True, vmem_limit_bytes=50_000_000
        ),
        name="layer",
    )(*(
        pltpu.with_memory_space_constraint(a, pltpu.HBM)
        for a in (
            lambdas, queries[0], keys[0], values[0], value_gain.reshape(1, 128),
            jnp.asarray(inner), jnp.asarray(outer), out_weight.T,
        )
    ))
    return out[None]


def solution(mesh):
    return jax.shard_map(
        shards,
        mesh=mesh,
        in_specs=(
            P("dp", "sp", None),
            P("dp", "sp", None),
            P("dp", "sp", None),
            P(),
            P(),
            P(None, ("sp", "dp")),
        ),
        out_specs=P("dp", "sp", None),
        check_vma=False,
    )
```

```python
import functools

import jax
import jax.numpy as jnp
import numpy as np
from jax import lax
from jax.experimental import pallas as pl
from jax.experimental.pallas import tpu as pltpu
from jax.sharding import PartitionSpec as P

HEADS = 16
KV_HEADS = 4
HEAD_DIM = 64
VALUE_DIM = 128
D = 4096
SEQLEN = 2048
ROWS = 128
GROUP = HEADS // KV_HEADS
KT = 512
ROPE_BASE = 500000.0
OUTPUT_SCALE = 0.8
NORM_EPS = 1e-05
MESH = pl.DeviceIdType.MESH

COLOURS = ((0, 1024), (1024, 512), (1536, 512))

DIRECT = ()
ORDER = (
    "x20s", "x1s", "z1s", "y1s", "x300s", "rotk", "kvzs", "kvy0s", "rotq", "kvy0f", "kvz3w", "kvy3s", "qs",
    "kvz1w", "z1f", "kvy1s", "x20f", "x301s", "x1f", "x310s", "x303s", "y1f", "x330s", "kvz2w", "kvy2s",
    "x300f", "z1e", "z30s", "kvy3f", "x301f", "kvy1f", "x23s", "x310f", "x20e", "x302s", "x303f", "y1e",
    "y2s", "kvy2f", "z2s", "x21s", "x1e", "x22s", "x320s", "x330f", "x23f", "x331s", "x333s", "kvall", "at00",
    "z30f", "x302f", "at01", "at02", "y2f", "y33s", "z2f", "z33s", "at10", "x21f", "x313s", "x311s", "at11",
    "at12", "x331f", "x22f", "x323s", "y31s", "x321s", "z31s", "z30e", "at20", "x23e", "x332s", "x333f",
    "at21", "at22", "x313f", "y30s", "o1w", "at30", "y2e", "y32s", "at31", "at32", "x22e", "x322s", "y33f",
    "z2e", "z32s", "x21e", "x311f", "x302e", "x320f", "x312s", "x323f", "z33f", "x321f", "y31f", "x332f",
    "o2w", "y30f", "x322f", "z31f", "o3w", "acts", "y32f", "x312f", "z32f", "y33e", "z33e", "pxz0", "x332e",
    "y31e", "x322e", "z31e", "pxz1", "y30e", "py0", "sw0", "x312e", "px0", "z32e", "pz2", "sw1", "y32e",
    "py2", "sw2", "m0", "m1", "m2",
)


def rotation_tables():
    f32 = np.float32
    freqs = (f32(ROPE_BASE) ** (-np.arange(0, HEAD_DIM, 2, dtype=f32) / f32(HEAD_DIM))).astype(f32)
    lanes = np.tile(freqs.astype(np.float64), 4)
    inner = np.arange(ROWS)[:, None] * lanes[None]
    outer = (np.arange(SEQLEN // ROWS) * ROWS)[:, None] * lanes[None]
    inner = np.stack([np.cos(inner), np.sin(inner)]).astype(f32)
    outer = np.stack([np.cos(outer), np.sin(outer)], 1).astype(f32)
    return inner, outer


def kernel(
    lam_hbm, q_hbm, k_hbm, v_hbm, gain_hbm, inner_hbm, outer_hbm, w_hbm,
    out_ref,
    lam_ref, gain_ref, inner_ref, outer_ref, q_in, k_in, v_in,
    kvst, kv, qst, qin, q2, sbuf, acc, wbuf, hst, acts, pacc, oown, opart, oin,
    in_sem, sent, kvz_r, kvy_r, q_r, ring_r, fin_r, oz_r, af_r, oo_r,
):
    f32, bf16 = jnp.float32, jnp.bfloat16
    sp, dp = lax.axis_index("sp"), lax.axis_index("dp")
    me = {"z": sp // 4, "y": lax.rem(sp, 4), "x": dp // 2}
    core = lax.rem(dp, 2)

    def at(pos):
        return (pos["z"] * 4 + pos["y"], pos["x"] * 2 + core)

    def shift(dim, off):
        return {**me, dim: lax.rem(me[dim] + off + 4, 4)}

    partner = (sp, me["x"] * 2 + 1 - core)
    total_sent = [0, 0]

    def size(ref):
        return int(np.prod(ref.shape)) * ref.dtype.itemsize

    def amount(nbytes):
        rows = nbytes // 4096
        n = 1 if rows <= KT else (2 if rows % 16 == 0 and rows <= 2 * KT else 4)
        assert rows * 4096 == nbytes and rows % n == 0
        return sbuf.at[pl.ds(0, n), pl.ds(0, rows // n), :]

    def send(src, dst, r_sem, dev, kind=0):
        total_sent[kind] += size(src)
        pltpu.make_async_remote_copy(
            src_ref=src, dst_ref=dst, send_sem=sent.at[kind], recv_sem=r_sem, device_id=dev, device_id_type=MESH
        ).start()

    def arrived(nbytes, r_sem, name="wait"):
        view = amount(nbytes)
        with jax.named_scope(name):
            pltpu.make_async_remote_copy(
                src_ref=view, dst_ref=view, send_sem=sent.at[0], recv_sem=r_sem, device_id=partner, device_id_type=MESH
            ).wait_recv()

    barrier = pltpu.get_barrier_semaphore()
    peers = [at(shift("z", o)) for o in (1, 2, 3)] + [at(shift("y", o)) for o in ((1, 2, 3) if DIRECT else (1, 3))]
    peers += [at(shift("x", o)) for o in (1, 3)] + [partner]
    for dev in peers:
        pl.semaphore_signal(barrier, inc=1, device_id=dev, device_id_type=MESH)

    copies = [
        pltpu.make_async_copy(src, dst, in_sem.at[n])
        for n, (src, dst) in enumerate((
            (k_hbm, k_in),
            (inner_hbm, inner_ref),
            (outer_hbm.at[sp], outer_ref),
            (v_hbm, v_in),
            (w_hbm, wbuf.at[me["z"], me["y"], me["x"]]),
            (q_hbm, q_in),
            (gain_hbm, gain_ref),
            (lam_hbm, lam_ref),
        ))
    ]
    for c in copies:
        c.start()
    c_k, c_in, c_out, c_v, c_w, c_q, c_gain, c_lam = copies
    with jax.named_scope("barrier"):
        pl.semaphore_wait(barrier, len(peers))

    def rotate(part):
        turned = jnp.dot(part, kept["swap"], preferred_element_type=f32)
        return (part.astype(f32) * kept["cosine"] + turned * kept["sine"]).astype(bf16)

    kept = {}

    def rotate_keys():
        with jax.named_scope("rotk"):
            row = lax.broadcasted_iota(jnp.int32, (128, 128), 0)
            col = lax.broadcasted_iota(jnp.int32, (128, 128), 1)
            low = lax.rem(col, 64) < 32
            kept["swap"] = jnp.where(
                low & (row == col + 32), -1.0, jnp.where(jnp.logical_not(low) & (row == col - 32), 1.0, 0.0)
            ).astype(bf16)
            c_v.wait()
            for g in range(KV_HEADS):
                kvst[g, 1] = v_in[:, g * 128:(g + 1) * 128].astype(f32).T.astype(bf16)
            c_in.wait()
            c_out.wait()
            ci, si = inner_ref[0], inner_ref[1]
            co, so = outer_ref[0:1, :], outer_ref[1:2, :]
            kept["cosine"] = co * ci - so * si
            kept["sine"] = so * ci + co * si
            c_k.wait()
            for g in range(KV_HEADS):
                kvst[g, 0] = rotate(k_in[:, g * 128:(g + 1) * 128])
            kv[sp, 0] = kvst[me["z"], 0]
            kv[sp, 1] = kvst[me["z"], 1]
            c_w.wait()

    steps = (0, 3, 1, 2)
    block_bytes = size(kv.at[0])

    def kv_block(rel, off):
        return lax.rem(me["z"] + rel, 4) * 4 + lax.rem(me["y"] + off + 4, 4)

    def kvz_start(o):
        pos = shift("z", o)
        send(kvst.at[pos["z"]], kv.at[sp], kvz_r.at[o - 1], at(pos))

    def kvz_wait(rel):
        arrived(block_bytes, kvz_r.at[3 - rel], f"kvz_{rel}")

    def kvy_start(rel):
        view = kvst.at[me["z"]] if rel == 0 else kv.at[kv_block(rel, 0)]
        for off in (1, -1):
            send(view, kv.at[kv_block(rel, 0)], kvy_r.at[4 if rel in DIRECT else rel], at(shift("y", off)))
        if rel in DIRECT:
            send(view, kv.at[kv_block(rel, 0)], kvy_r.at[4], at(shift("y", 2)))

    def kvy_forward(rel):
        arrived(2 * block_bytes, kvy_r.at[rel], f"kvy_{rel}")
        for n, off in enumerate((-1, 1)):
            half = kv.at[kv_block(rel, off), n]
            send(half, half, kvy_r.at[4], at(shift("y", -off)))

    made = []

    class Ring:
        def __init__(self, colour, dim, fin, **fixed):
            self.dim, self.fixed = dim, fixed
            self.k0, self.kn = COLOURS[colour]
            self.full, self.fin = ring_r.at[len(made)], fin_r.at[fin]
            self.bytes = size(self.view(0))
            self.name = f"{len(made)}{dim}"
            made.append(self)

        def view(self, off, half=None):
            sel, rows = {}, slice(None)
            for d in "zyx":
                rel = off if d == self.dim else self.fixed[d]
                sel[d] = slice(None) if rel is None else lax.rem(me[d] + rel + 4, 4)
            if half is not None:
                free = [d for d in "zyx" if d != self.dim and self.fixed[d] is None]
                if free:
                    sel[free[0]] = pl.ds(2 * half, 2)
                else:
                    rows = pl.ds(16 * half, 16)
            return wbuf.at[sel["z"], sel["y"], sel["x"], rows, pl.ds(self.k0, self.kn)]

        def start(self):
            view = src = self.view(0)
            if all(r == 0 for r in self.fixed.values()):
                src = w_hbm.at[:, pl.ds(self.k0, self.kn)]
            for off in (1, -1):
                send(src, view, self.full, at(shift(self.dim, off)), 1)

        def forward(self):
            arrived(2 * self.bytes, self.full, "fwd" + self.name)
            for n, off in enumerate((-1, 1)):
                half = self.view(off, n)
                send(half, half, self.fin, at(shift(self.dim, -off)), 1)

        def finish(self):
            arrived(self.bytes, self.fin, "fin" + self.name)

    x1 = Ring(0, "z", 0, y=0, x=0)
    x2 = {a: Ring(0, "y", 1 + a, z=a, x=0) for a in steps}
    x3 = {(a, b): Ring(0, "x", 21 + a if b == 2 else 5 + b, z=a, y=b) for b in steps for a in steps}
    y1 = Ring(1, "x", 9, z=0, y=0)
    y2 = Ring(1, "z", 10, x=None, y=0)
    y3 = {a: Ring(1, "y", 11 + a, x=None, z=a) for a in steps}
    z1 = Ring(2, "x", 15, z=0, y=0)
    z2 = Ring(2, "y", 16, x=None, z=0)
    z3 = {b: Ring(2, "z", 17 + b, x=None, y=b) for b in steps}

    def x3_finish(b):
        arrived(4 * x3[0, b].bytes, x3[0, b].fin, f"finx{b}")

    tasks = {"kvzs": lambda: [kvz_start(o) for o in (1, 3, 2)]}
    for a in steps:
        tasks[f"kvz{a}w"] = functools.partial(kvz_wait, a)
        tasks[f"kvy{a}s"] = functools.partial(kvy_start, a)
        if a not in DIRECT:
            tasks[f"kvy{a}f"] = functools.partial(kvy_forward, a)
    tasks["kvall"] = lambda: arrived((4 + 2 * len(DIRECT)) * block_bytes, kvy_r.at[4], "kvyf")
    rings = {"x1": x1, "y1": y1, "z1": z1, "y2": y2, "z2": z2}
    for a in steps:
        rings.update({f"x2{a}": x2[a], f"y3{a}": y3[a], f"z3{a}": z3[a]})
        rings.update({f"x3{a}{b}": x3[a, b] for b in steps})
    for name, ring in rings.items():
        tasks.update({name + "s": ring.start, name + "f": ring.forward, name + "e": ring.finish})

    def rotate_queries():
        with jax.named_scope("rotq"):
            c_q.wait()
            for g in range(KV_HEADS):
                for h in range(GROUP):
                    a = (g * GROUP + h) * 128
                    qst[g, :, h * 128:(h + 1) * 128] = rotate(q_in[:, a:a + 128])
            qin[me["z"]] = qst[me["z"]]
            pacc[...] = jnp.zeros_like(pacc)

    def send_queries():
        for o in (1, 3, 2):
            pos = shift("z", o)
            send(qst.at[pos["z"]], qin.at[me["z"]], q_r.at[o - 1], at(pos))

    tasks.update({"rotk": rotate_keys, "rotq": rotate_queries, "qs": send_queries})

    scale = float(HEAD_DIM ** -0.5 * np.log2(np.e))
    half_rows = GROUP * ROWS

    def fold(x, op):
        return op(x.reshape(KT // 8, 8, x.shape[1]), 0)

    def attend_scores(i):
        zq = lax.rem(me["z"] + 1 + i, 4)
        if i < 3:
            o = 3 - i
            arrived(size(qin.at[0]), q_r.at[o - 1], f"q_{i}")
        lane = lax.broadcasted_iota(jnp.int32, (128, 128), 1)
        for m in range(2):
            keep = (lane < 64) if m == 0 else (lane >= 64)
            for h in range(GROUP):
                part = qin[zq, :, h * 128:(h + 1) * 128]
                q2[(m * GROUP + h) * 128:(m * GROUP + h + 1) * 128, :] = jnp.where(
                    keep, part, jnp.zeros_like(part)
                )
        block = zq * 4 + me["y"]
        last = zq

        def scores(t):
            keys = jnp.concatenate([kv[4 * t + b, 0] for b in range(4)], 0)
            return lax.dot_general(keys, q2[...], (((1,), (1,)), ((), ())), preferred_element_type=f32)

        def pass1(t, top):
            s = scores(t)
            sbuf[t] = s
            return jnp.maximum(top, fold(s, jnp.max))

        top = lax.fori_loop(0, last, pass1, jnp.full((8, 2 * half_rows), -1e30, f32))
        s = scores(last)
        key_at = lax.broadcasted_iota(jnp.int32, (KT, 2 * half_rows), 0) + last * KT
        query_at = lax.rem(lax.broadcasted_iota(jnp.int32, (KT, 2 * half_rows), 1), 128) + block * 128
        s = jnp.where(key_at <= query_at, s, -1e30)
        sbuf[last] = s
        top = jnp.maximum(top, fold(s, jnp.max))
        top = jnp.max(top, 0, keepdims=True)
        kept["top"] = top

    def attend_exp(i):
        last = lax.rem(me["z"] + 1 + i, 4)
        top = kept["top"]

        def pass2(t, total):
            p = jnp.exp2((sbuf[t] - top) * scale)
            sbuf[t] = p
            return total + fold(p, jnp.sum)

        total = lax.fori_loop(0, last + 1, pass2, jnp.zeros((8, 2 * half_rows), f32))
        kept["total"] = jnp.sum(total, 0, keepdims=True)

    def attend_values(i):
        zq = last = lax.rem(me["z"] + 1 + i, 4)
        total = kept["total"]
        if i == 0:
            c_lam.wait()
            c_gain.wait()
        lam = jnp.concatenate(
            [jnp.full((1, 128), lam_ref[me["z"] * GROUP + h], f32) for h in range(GROUP)], 1
        )
        a0 = 1.0 / total[:, :half_rows]
        a1 = lam / total[:, half_rows:]
        acc[...] = jnp.zeros_like(acc)

        def pass3(t, carry):
            w = (sbuf[t, :, :half_rows] * a0 - sbuf[t, :, half_rows:] * a1).astype(bf16)
            vals = jnp.concatenate([kv[4 * t + b, 1] for b in range(4)], 1)
            acc[...] += jnp.dot(vals, w, preferred_element_type=f32)
            return carry

        lax.fori_loop(0, last + 1, pass3, 0)
        hv = acc[...]
        inv = lax.rsqrt(jnp.mean(hv * hv, 0, keepdims=True) + NORM_EPS)
        hv = hv * inv
        for h in range(GROUP):
            piece = hv[:, h * 128:(h + 1) * 128].T
            hst[zq, :, h * 128:(h + 1) * 128] = (piece * gain_ref[...] * OUTPUT_SCALE).astype(bf16)
        ship(i, zq)

    def ship(i, zq):
        if i < 3:
            o = i + 1
            send(hst.at[zq], acts.at[0, me["z"]], oz_r.at[o - 1], at(shift("z", o)))
        else:
            acts[0, me["z"]] = hst[me["z"]]
            send(hst.at[me["z"]], acts.at[1, me["z"]], af_r.at[0], partner)

    def acts_in(o):
        g = lax.rem(me["z"] + 4 - o, 4)
        arrived(size(acts.at[0, 0]), oz_r.at[o - 1], f"o_{o}")
        send(acts.at[0, g], acts.at[1, g], af_r.at[0], partner)

    def multiply(heads, weights):
        total = None
        for n, g in enumerate(heads):
            part = lax.dot_general(
                acts[:, g].reshape(2 * ROWS, 512), weights[:, n * 512:(n + 1) * 512],
                (((1,), (1,)), ((), ())), preferred_element_type=f32,
            )
            total = part if total is None else total + part
        return total

    def project_xz(places):
        with jax.named_scope(f"proj_xz{places[0]}"):
            spots = [(z, lax.rem(me["y"] + b, 4)) for b in places for z in range(4)]
            cat = lambda lo, hi: jnp.concatenate(
                [wbuf[z, y, :, :, lo:hi].reshape(128, hi - lo) for z, y in spots], 0
            )
            part = multiply((0, 1), cat(0, 1024)) + multiply((3,), cat(1536, 2048))
            for n, (z, y) in enumerate(spots):
                pacc[z, y] += part[:, n * 128:(n + 1) * 128]

    def project_x(places):
        with jax.named_scope(f"proj_x{places[0]}"):
            spots = [tile_of(a, 2) for a in places]
            cat = jnp.concatenate([wbuf[z, y, :, :, 0:1024].reshape(128, 1024) for z, y in spots], 0)
            part = multiply((0, 1), cat)
            for n, (z, y) in enumerate(spots):
                pacc[z, y] += part[:, n * 128:(n + 1) * 128]

    def project_z(b):
        with jax.named_scope(f"proj_z{b}"):
            yb = lax.rem(me["y"] + b, 4)
            cat = jnp.concatenate([wbuf[z, yb, :, :, 1536:2048].reshape(128, 512) for z in range(4)], 0)
            part = multiply((3,), cat)
            for z in range(4):
                pacc[z, yb] += part[:, z * 128:(z + 1) * 128]

    def project_y(places):
        with jax.named_scope(f"proj_y{places[0]}"):
            spots = [lax.rem(me["z"] + a, 4) for a in places]
            cat = jnp.concatenate([wbuf[z, :, :, :, 1024:1536].reshape(512, 512) for z in spots], 0)
            part = multiply((2,), cat)
            for n, z in enumerate(spots):
                for y in range(4):
                    pacc[z, y] += part[:, (n * 4 + y) * 128:(n * 4 + y + 1) * 128]

    early = [(a, b) for a in (0, 3, 1) for b in (0, 3, 1)]
    late = [(a, 2) for a in (0, 3, 1)]

    def tile_of(a, b):
        return lax.rem(me["z"] + a, 4), lax.rem(me["y"] + b, 4)

    def swap_tiles(tiles, n):
        for a, b in tiles:
            z, y = tile_of(a, b)
            opart[z, y] = pacc[z, y, ROWS:].astype(bf16)
        for a, b in tiles:
            z, y = tile_of(a, b)
            send(opart.at[z, y], oin.at[z, y], oo_r.at[n], partner)
            oown[z, y] = pacc[z, y, :ROWS].astype(bf16)

    def spread():
        erow = lax.broadcasted_iota(jnp.int32, (256, 256), 0)
        ecol = lax.broadcasted_iota(jnp.int32, (256, 256), 1)
        mine = jnp.where(erow < 128, core, 1 - core)
        er = lax.rem(erow, 128)
        return jnp.where(ecol == (er // 32) * 64 + mine * 32 + lax.rem(er, 32), 1.0, 0.0).astype(bf16)

    def merge(tiles, n):
        arrived(len(tiles) * size(oin.at[0, 0]), oo_r.at[n], f"swap_{n}")
        with jax.named_scope(f"merge_{n}"):
            if n == 0:
                kept["spread"] = spread()
            for a, b in tiles:
                z, y = tile_of(a, b)
                both = jnp.concatenate([oown[z, y], oin[z, y]], 1)
                cols = pl.ds(pl.multiple_of((z * 4 + y) * 256, 256), 256)
                out_ref[:, cols] = jnp.dot(both, kept["spread"], preferred_element_type=f32).astype(bf16)

    def scoped(name, fn, *args):
        with jax.named_scope(name):
            fn(*args)

    def project_xz_task(places):
        for b in places:
            x3_finish(b)
        project_xz(places)

    for i in range(4):
        for n, fn in enumerate((attend_scores, attend_exp, attend_values)):
            tasks[f"at{i}{n}"] = functools.partial(scoped, f"at{i}{n}", fn, i)
    for o in (1, 2, 3):
        tasks[f"o{o}w"] = functools.partial(acts_in, o)
    tasks["acts"] = lambda: arrived(4 * size(acts.at[0, 0]), af_r.at[0], "acts")
    tasks["pxz0"] = functools.partial(project_xz_task, (0, 3))
    tasks["pxz1"] = functools.partial(project_xz_task, (1,))
    tasks["py0"] = functools.partial(project_y, (0, 3, 1))
    tasks["py2"] = functools.partial(project_y, (2,))
    tasks["px0"] = functools.partial(project_x, steps)
    tasks["pz2"] = functools.partial(project_z, 2)
    for n, tiles in enumerate((early, late, [(2, b) for b in steps])):
        tasks[f"sw{n}"] = functools.partial(swap_tiles, tiles, n)
        tasks[f"m{n}"] = functools.partial(merge, tiles, n)
    left = [n for n in tasks if not (n.startswith("x3") and n.endswith("e") and n[3] != "2")]
    left.remove("kvz0w")
    assert sorted(left) == sorted(ORDER)
    for name in ORDER:
        tasks[name]()
    with jax.named_scope("drain"):
        for kind in (0, 1):
            view = amount(total_sent[kind])
            pltpu.make_async_remote_copy(
                src_ref=view, dst_ref=view, send_sem=sent.at[kind], recv_sem=oo_r.at[0],
                device_id=partner, device_id_type=MESH,
            ).wait_send()


def shards(queries, keys, values, lambdas, value_gain, out_weight):
    inner, outer = rotation_tables()
    vmem = pl.BlockSpec(memory_space=pltpu.VMEM)
    hbm = pl.BlockSpec(memory_space=pltpu.HBM)
    bf16, f32 = jnp.bfloat16, jnp.float32
    dma = lambda n: pltpu.SemaphoreType.DMA((n,))
    out = pl.pallas_call(
        kernel,
        out_shape=jax.ShapeDtypeStruct((ROWS, D), bf16),
        in_specs=[hbm] * 8,
        out_specs=vmem,
        scratch_shapes=[
            pltpu.SMEM((HEADS,), f32),
            pltpu.VMEM((1, 128), f32),
            pltpu.VMEM((2, ROWS, 128), f32),
            pltpu.VMEM((2, 128), f32),
            pltpu.VMEM((ROWS, 2048), bf16),
            pltpu.VMEM((ROWS, 512), bf16),
            pltpu.VMEM((ROWS, 512), bf16),
            pltpu.VMEM((4, 2, 128, 128), bf16),
            pltpu.VMEM((16, 2, 128, 128), bf16),
            pltpu.VMEM((4, 128, 512), bf16),
            pltpu.VMEM((4, 128, 512), bf16),
            pltpu.VMEM((1024, 128), bf16),
            pltpu.VMEM((SEQLEN // KT, KT, 1024), f32),
            pltpu.VMEM((128, 512), f32),
            pltpu.VMEM((4, 4, 4, 32, 2048), bf16),
            pltpu.VMEM((4, 128, 512), bf16),
            pltpu.VMEM((2, 4, 128, 512), bf16),
            pltpu.VMEM((4, 4, 256, 128), f32),
            pltpu.VMEM((4, 4, 128, 128), bf16),
            pltpu.VMEM((4, 4, 128, 128), bf16),
            pltpu.VMEM((4, 4, 128, 128), bf16),
            dma(8), dma(2), dma(3), dma(5), dma(3), dma(33), dma(25), dma(3), dma(1), dma(3),
        ],
        compiler_params=pltpu.CompilerParams(
            collective_id=0, has_side_effects=True, vmem_limit_bytes=50_000_000
        ),
        name="layer",
    )(*(
        pltpu.with_memory_space_constraint(a, pltpu.HBM)
        for a in (
            lambdas, queries[0], keys[0], values[0], value_gain.reshape(1, 128),
            jnp.asarray(inner), jnp.asarray(outer), out_weight.T,
        )
    ))
    return out[None]


def solution(mesh):
    return jax.shard_map(
        shards,
        mesh=mesh,
        in_specs=(
            P("dp", "sp", None),
            P("dp", "sp", None),
            P("dp", "sp", None),
            P(),
            P(),
            P(None, ("sp", "dp")),
        ),
        out_specs=P("dp", "sp", None),
        check_vma=False,
    )
```
